256 devices in a mesh: sp: 16 (over y, x), tp: 16 (over z, core).
Axes of the slice: x: 4, y: 4, z: 8, core: 2. Of those that a mesh axis runs over, the one named last changes fastest.
Arguments:
- conv_value: bfloat16 [49152, 2048], P('sp', 'tp'), may hold values from -48 to 48
- conv_gate: bfloat16 [49152, 2048], P('sp', 'tp'), may hold values from -6 to 6
- doc_ids: int32 [49152], P('sp'), may hold values from 0 to 15, never falling along the last dimension, each value on 1 to 9216 neighbouring positions
- conv_kernel: bfloat16 [31, 2048], P(None, 'tp'), may hold values from -1 to 1
- norm_gain_conv: float32 [2048], replicated, may hold values from 0.1 to 1.9
- norm_bias_conv: float32 [2048], replicated, may hold values from -3 to 3
- proj_weight: bfloat16 [2048, 2048], P('tp'), may hold values from -0.125 to 0.125
- residual: bfloat16 [49152, 2048], P(('sp', 'tp')), may hold values from -6 to 6
- norm_gain_moe: float32 [2048], replicated, may hold values from 0.1 to 1.9
- group_router: bfloat16 [2048, 2], replicated, may hold values from -0.125 to 0.125
- expert_router: bfloat16 [2048, 16], replicated, may hold values from -0.125 to 0.125
- routing: int32 [49152, 2], P(('sp', 'tp')), may hold values from 0 to 15, as said below
- expert_gate_w: bfloat16 [16, 2048, 512], P('sp'), may hold values from -0.125 to 0.125
- expert_up_w: bfloat16 [16, 2048, 512], P('sp'), may hold values from -0.125 to 0.125
- expert_down_w: bfloat16 [16, 512, 2048], P('sp'), may hold values from -0.25 to 0.25
Outputs:
- output: bfloat16 [49152, 2048], P(('sp', 'tp'))
The draws below stay inside these ranges and needn't reach their ends.
Inputs may be any that keep to these rules, and one draw needn't show every extreme that they name: `routing`: both numbers of a row are different experts of one group (expert // 8); within the rows of one device (aligned blocks of 192 rows) every expert is named exactly 24 times.
All inputs are finite; a program needn't handle non-finite values.
Results may differ from the reference program's by a relative error of at most 0.015.
Values may be sent and summed in bfloat16 or wider, within the bound.
A program may use at most 64 MiB of HBM per device.

```python
import math
import jax
import jax.numpy as jnp
import numpy as np
from jax import lax

D = 2048
CH = 2048
KW = 31
FF = 512
GROUPS = 2
TOK_DEV = 192
EXPERTS = 16
TOKENS = 49152
DOCS = 16
DOC_MOST = 9216


def draw_conv_value(key, part):
    base_key = jax.random.fold_in(key, 101)
    column_key = jax.random.fold_in(key, 102)
    column_scale = 3.0 ** (jnp.arange(CH, dtype=jnp.float32) / CH) * jax.random.uniform(column_key, (CH,), jnp.float32, 0.6, 1.6)
    base = jnp.clip(jax.random.normal(base_key, (TOKENS, CH), jnp.float32), -6.0, 6.0)
    return (base * column_scale[None, :]).astype(jnp.bfloat16)


def draw_routing(key, part):
    blocks = TOKENS // TOK_DEV
    per_group = EXPERTS // GROUPS
    group_rows = TOK_DEV // GROUPS
    per_expert = TOK_DEV // EXPERTS
    shift_key = jax.random.fold_in(key, 201)
    flip_key = jax.random.fold_in(key, 202)
    shuffle_key = jax.random.fold_in(key, 203)
    rank_order = jnp.arange(TOK_DEV, dtype=jnp.int32)
    first_local = rank_order % group_rows // per_expert
    shifts = jax.random.randint(shift_key, (blocks,), 1, per_group, jnp.int32)
    flips = jax.random.randint(flip_key, (blocks,), 0, GROUPS, jnp.int32)
    group_index = (rank_order[None, :] // group_rows + flips[:, None]) % GROUPS
    second_local = (first_local[None, :] + shifts[:, None]) % per_group
    first_expert = group_index * per_group + first_local[None, :]
    second_expert = group_index * per_group + second_local
    pairing = jnp.stack([first_expert, second_expert], axis=-1).astype(jnp.int32)
    shuffles = jax.vmap(lambda block_key: jax.random.permutation(block_key, TOK_DEV))(jax.random.split(shuffle_key, blocks))

    def place_block(shuffle, block_pairs):
        return jnp.zeros((TOK_DEV, 2), jnp.int32).at[shuffle].set(block_pairs)
    routed = jax.vmap(place_block)(shuffles.astype(jnp.int32), pairing)
    return routed.reshape(TOKENS, 2).astype(jnp.int32)


def shard_levels(key, dims, cuts, smallest, high):
    loudness, own = 1.0, jax.random.fold_in(key, 6)
    for axis_at, shards_of in cuts:
        steps = jnp.exp(jax.random.uniform(jax.random.fold_in(own, axis_at), (shards_of,), jnp.float32, smallest / len(cuts), high / len(cuts)))
        loudness = loudness * jnp.repeat(steps, dims[axis_at] // shards_of).reshape([-1 if axis == axis_at else 1 for axis in range(len(dims))])
    return loudness


def length_profile(count, total, reach, lean):
    portions = [(1 << 20) // math.isqrt(grade ** lean) + 1 for grade in range(2, count + 1)]
    surplus, given = total - reach - (count - 1), [1] * (count - 1)
    while surplus > 0:
        movable = [i for i in range(count - 1) if given[i] < reach]
        mass, budget = sum([portions[i] for i in movable]), surplus
        for i in movable:
            more = min(reach - given[i], max(1, budget * portions[i] // mass), surplus)
            given[i] = given[i] + more
            surplus = surplus - more
    return np.array([reach] + given)


def ragged_sizes(rng, number_of, total, limit, skew):
    if number_of == 2:
        one = jax.random.randint(rng, (), max(1, total - limit), min(limit, total - 1) + 1)
        return jnp.stack([one, total - one])
    tallies = jnp.asarray(length_profile(number_of, total, limit, skew), jnp.int32)
    couples = (number_of - 1) // 2
    donor, taker = tallies[1:1 + 2 * couples:2], tallies[2:2 + 2 * couples:2]
    room = jnp.minimum(donor - 1, limit - taker)
    moved = jax.random.randint(jax.random.fold_in(rng, 1), (couples,), 0, 1 << 20) % (room + 1)
    tallies = tallies.at[1:1 + 2 * couples:2].set(donor - moved).at[2:2 + 2 * couples:2].set(taker + moved)
    return tallies[jax.random.permutation(jax.random.fold_in(rng, 2), number_of)]


def normal_values(key, extent, spread, limit, cuts=(), kind=jnp.bfloat16):
    array = jax.random.normal(key, extent, jnp.float32) * spread
    if len(cuts) > 0:
        array = shard_levels(key, extent, cuts, -0.22, 0.18) * array
    return jnp.clip(array, min=-limit, max=limit).astype(kind)


def setup_inputs(seed: int = 0) -> dict:
    seeds = jax.random.split(jax.random.key(seed), 16)
    return {
        "conv_value": draw_conv_value(jax.random.fold_in(seeds[15], 71), 0),
        "conv_gate": normal_values(seeds[1], (TOKENS, CH), 1.0, 6.0, ((0, 16), (1, 16))),
        "doc_ids": jnp.searchsorted(jnp.cumsum(ragged_sizes(seeds[2], DOCS, TOKENS, DOC_MOST, 0)), jnp.arange(TOKENS), side="right").astype(jnp.int32),
        "conv_kernel": normal_values(seeds[3], (KW, CH), KW ** -0.5, 1.0, ((1, 16),)),
        "norm_gain_conv": jnp.clip(1.0 + 0.18 * jax.random.normal(seeds[4], (CH,), jnp.float32), 0.1, 1.9),
        "norm_bias_conv": normal_values(seeds[5], (CH,), 0.5, 3.0, (), jnp.float32),
        "proj_weight": normal_values(seeds[6], (CH, D), CH ** -0.5, 0.125, ((0, 16),)),
        "residual": normal_values(seeds[7], (TOKENS, D), 1.0, 6.0, ((0, 256),)),
        "norm_gain_moe": jnp.clip(1.0 + 0.18 * jax.random.normal(seeds[8], (D,), jnp.float32), 0.1, 1.9),
        "group_router": normal_values(seeds[9], (D, GROUPS), D ** -0.5, 0.125),
        "expert_router": normal_values(seeds[10], (D, EXPERTS), D ** -0.5, 0.125),
        "routing": draw_routing(jax.random.fold_in(seeds[15], 71), 0),
        "expert_gate_w": normal_values(seeds[12], (EXPERTS, D, FF), D ** -0.5, 0.125, ((0, 16),)),
        "expert_up_w": normal_values(seeds[13], (EXPERTS, D, FF), D ** -0.5, 0.125, ((0, 16),)),
        "expert_down_w": normal_values(seeds[14], (EXPERTS, FF, D), FF ** -0.5, 0.25, ((0, 16),)),
    }


epsilon = 1e-06

def reference(conv_value, conv_gate, doc_ids, conv_kernel, norm_gain_conv, norm_bias_conv, proj_weight, residual, norm_gain_moe, group_router, expert_router, routing, expert_gate_w, expert_up_w, expert_down_w):
    gated_values = (conv_value.astype(jnp.float32) * jax.nn.sigmoid(conv_gate.astype(jnp.float32))).astype(jnp.bfloat16)
    rim_width = KW - 1
    length = gated_values.shape[0]
    padded = jnp.concatenate([jnp.zeros((rim_width, CH), jnp.bfloat16), gated_values], axis=0)
    padded_ids = jnp.concatenate([jnp.zeros((rim_width,), jnp.int32), doc_ids.astype(jnp.int32)], axis=0)
    kernel = conv_kernel.astype(jnp.float32)
    summed = jnp.zeros((length, CH), jnp.float32)
    for tap in range(KW):
        same_doc = padded_ids[tap:tap + length] == doc_ids
        summed = summed + jnp.where(same_doc[:, None], padded[tap:tap + length].astype(jnp.float32) * kernel[tap][None, :], jnp.float32(0.0))
    convolved = summed.astype(jnp.bfloat16)
    values = convolved.astype(jnp.float32)
    average = lax.optimization_barrier(jnp.mean(values, axis=1, keepdims=True))
    centered = values - average
    variance = lax.optimization_barrier(jnp.mean(centered * centered, axis=1, keepdims=True))
    activated = jax.nn.silu(centered * lax.rsqrt(variance + epsilon) * norm_gain_conv + norm_bias_conv).astype(jnp.bfloat16)
    projected = jnp.dot(activated, proj_weight, preferred_element_type=jnp.float32)
    hidden_state = (residual.astype(jnp.float32) + projected).astype(jnp.bfloat16)
    state_values = hidden_state.astype(jnp.float32)
    normed = (state_values * lax.rsqrt(lax.optimization_barrier(jnp.mean(state_values * state_values, axis=1, keepdims=True)) + epsilon) * norm_gain_moe).astype(jnp.bfloat16)
    group_logits = jnp.dot(normed, group_router, preferred_element_type=jnp.float32)
    expert_logits = jnp.dot(normed, expert_router, preferred_element_type=jnp.float32)
    per_group = EXPERTS // GROUPS
    chosen_group = (routing[:, 0] // per_group).astype(jnp.int32)
    group_exp = jnp.exp(group_logits)
    group_prob = jnp.take_along_axis(group_exp, chosen_group[:, None], axis=1)[:, 0] / lax.optimization_barrier(jnp.sum(group_exp, axis=1))
    first_logit = jnp.take_along_axis(expert_logits, routing[:, 0:1], axis=1)[:, 0]
    second_logit = jnp.take_along_axis(expert_logits, routing[:, 1:2], axis=1)[:, 0]
    first_exp = jnp.exp(first_logit)
    second_exp = jnp.exp(second_logit)
    first_weight = group_prob * first_exp / (first_exp + second_exp)
    second_weight = group_prob * second_exp / (first_exp + second_exp)
    per_expert = 2 * length // EXPERTS
    flat_experts = routing.reshape(-1).astype(jnp.int32)
    ordering = jnp.argsort(flat_experts, stable=True).astype(jnp.int32)
    slot_table = ordering.reshape(EXPERTS, per_expert)

    def one_expert(operands):
        assigned, gate_matrix, up_matrix, down_matrix = operands
        token_rows = normed[assigned // 2]
        gate_part = jnp.dot(token_rows, gate_matrix, preferred_element_type=jnp.float32)
        up_part = jnp.dot(token_rows, up_matrix, preferred_element_type=jnp.float32)
        expert_hidden = (jax.nn.silu(gate_part) * up_part).astype(jnp.bfloat16)
        return jnp.dot(expert_hidden, down_matrix, preferred_element_type=jnp.float32).astype(jnp.bfloat16)
    results = lax.map(one_expert, (slot_table, expert_gate_w, expert_up_w, expert_down_w))
    per_assignment = jnp.zeros((2 * length, D), jnp.bfloat16).at[slot_table.reshape(-1)].set(results.reshape(-1, D))
    picked = per_assignment.reshape(length, 2, D).astype(jnp.float32)
    mixture = first_weight[:, None] * picked[:, 0] + second_weight[:, None] * picked[:, 1]
    return (state_values + mixture).astype(jnp.bfloat16)
```

```python
import functools
import jax
import jax.numpy as jnp
from jax import lax
from jax.experimental import pallas as pl
from jax.experimental.pallas import tpu as pltpu
from jax.sharding import PartitionSpec as P

epsilon = 1e-06
MESH = pl.DeviceIdType.MESH
F32 = jnp.float32
BF16 = jnp.bfloat16


def conv_kernel(
    sp_size, tp_size, value_ref, gate_ref, ids_ref, taps_ref, raw_ref,
    gated, reach, compact, outgoing, halo_ids, taps_wide,
    send_sem, recv_sem, halo_send, halo_recv,
):
    s = lax.axis_index("sp")
    t = lax.axis_index("tp")
    planes = tp_size // 2
    z, core = t // 2, t % 2
    rows, width = value_ref.shape
    block = rows // tp_size
    taps = taps_ref.shape[0]
    after, before = (s + 1) % sp_size, (s + sp_size - 1) % sp_size

    barrier = pltpu.get_barrier_semaphore()

    def greet(i, carry):
        other = (t + 1 + i) % tp_size
        pl.semaphore_signal(barrier, inc=1, device_id=(s, other), device_id_type=MESH)
        return carry

    lax.fori_loop(0, tp_size - 1, greet, 0)
    pl.semaphore_signal(barrier, inc=1, device_id=(after, t), device_id_type=MESH)
    pl.semaphore_signal(barrier, inc=1, device_id=(before, t), device_id_type=MESH)

    def gate_rows(r, carry):
        at = pl.multiple_of(r * 128, 128)
        v = value_ref[pl.ds(at, 128), :].astype(F32)
        g = gate_ref[pl.ds(at, 128), :].astype(F32)
        gated[pl.ds(at + 32, 128), :] = (v * jax.nn.sigmoid(g)).astype(BF16).astype(F32)
        return carry

    chunks = rows // 128
    gate_rows(chunks - 1, 0)
    wide = taps_ref[...].astype(F32)
    for k in range(taps):
        taps_wide[k] = jnp.broadcast_to(wide[k : k + 1, :], (8, width))
    pl.semaphore_wait(barrier, tp_size + 1)
    halo = pltpu.make_async_remote_copy(
        src_ref=gated.at[pl.ds(rows, 32)], dst_ref=gated.at[pl.ds(0, 32)],
        send_sem=halo_send.at[0], recv_sem=halo_recv.at[0],
        device_id=(after, t), device_id_type=MESH,
    )
    halo.start()
    halo_id = pltpu.make_async_remote_copy(
        src_ref=ids_ref.at[pl.ds(chunks - 8, 8)], dst_ref=halo_ids,
        send_sem=halo_send.at[1], recv_sem=halo_recv.at[1],
        device_id=(after, t), device_id_type=MESH,
    )
    halo_id.start()
    lax.fori_loop(0, chunks - 1, gate_rows, 0)

    ids = ids_ref[...]
    lane = lax.broadcasted_iota(jnp.int32, (chunks, 128), 1)
    row = lax.broadcasted_iota(jnp.int32, (chunks, 128), 0)
    position = row * 128 + lane
    began = jnp.zeros((chunks, 128), jnp.int32)
    for d in range(1, 16):
        count = jnp.sum(
            jnp.sum((ids < d).astype(jnp.int32), axis=1, keepdims=True), axis=0, keepdims=True
        )
        began = jnp.where(ids == d, count, began)
    halo_id.wait()
    tail_lane = lax.broadcasted_iota(jnp.int32, (1, 128), 1)
    shared = (halo_ids[7:8, :] == ids[0:1, 0:1]) & (tail_lane >= 128 - (taps - 1))
    extra = jnp.sum(shared.astype(jnp.int32), axis=1, keepdims=True)
    extra = extra * (s > 0).astype(jnp.int32)
    distance = position - began + jnp.where(began == 0, extra, 0)
    compact[...] = jnp.minimum(distance, taps).astype(F32)
    eye = (
        lax.broadcasted_iota(jnp.int32, (128, 128), 0)
        == lax.broadcasted_iota(jnp.int32, (128, 128), 1)
    ).astype(F32)
    ones = jnp.ones((128, 128), BF16)

    def widen(r, carry):
        spread = (eye * compact[pl.ds(r, 1), :]).astype(BF16)
        reach[pl.ds(pl.multiple_of(r * 128, 128), 128), :] = jnp.dot(
            spread, ones, preferred_element_type=F32
        )
        return carry

    lax.fori_loop(0, chunks, widen, 0)
    halo.wait()

    tile = 32

    def conv_block(b, store):
        def conv_tile(q, carry):
            base = pl.multiple_of(b * block + q * tile, tile)
            limit = reach[pl.ds(base, tile), :].reshape(tile // 8, 8, width)
            total = jnp.zeros((tile // 8, 8, width), F32)
            for k in range(taps):
                j = taps - 1 - k
                x = gated[pl.ds(base + (32 - j), tile), :].reshape(tile // 8, 8, width)
                total = total + jnp.where(limit >= j, x * taps_wide[k][None], 0.0)
            store(pl.multiple_of(q * tile, tile), total.reshape(tile, width).astype(BF16))
            return carry

        lax.fori_loop(0, block // tile, conv_tile, 0)

    def target(i):
        k = i // 2
        size = planes // 2 - (k + 1) // 2
        hop = (k % 2) * size + (1 - k % 2) * (planes - size)
        return ((z + hop) % planes) * 2 + (core + 1 + i) % 2

    def exchange(i):
        to = target(i)
        return pltpu.make_async_remote_copy(
            src_ref=outgoing.at[to], dst_ref=raw_ref.at[t],
            send_sem=send_sem.at[i], recv_sem=recv_sem.at[t],
            device_id=(s, to), device_id_type=MESH,
        )

    def step(i, carry):
        b = target(i)

        def store(at, value):
            outgoing[b, pl.ds(at, tile), :] = value

        conv_block(b, store)

        @pl.when(i > 0)
        def _():
            exchange(i - 1).start()

        return carry

    lax.fori_loop(0, tp_size - 1, step, 0)

    def store_own(at, value):
        raw_ref[t, pl.ds(at, tile), :] = value

    conv_block(t, store_own)
    exchange(tp_size - 2).start()

    def finish(i, carry):
        exchange(i).wait_send()
        source = (t + 1 + i) % tp_size
        pltpu.make_async_remote_copy(
            src_ref=outgoing.at[source], dst_ref=raw_ref.at[source],
            send_sem=send_sem.at[i], recv_sem=recv_sem.at[source],
            device_id=(s, source), device_id_type=MESH,
        ).wait_recv()
        return carry

    lax.fori_loop(0, tp_size - 1, finish, 0)


def conv_exchange(mesh, conv_value, conv_gate, doc_ids, conv_kernel_taps):
    sp_size, tp_size = mesh.shape["sp"], mesh.shape["tp"]
    rows, width = conv_value.shape
    block = rows // tp_size
    taps = conv_kernel_taps.shape[0]
    vmem = pl.BlockSpec(memory_space=pltpu.VMEM)
    return pl.pallas_call(
        functools.partial(conv_kernel, sp_size, tp_size),
        out_shape=jax.ShapeDtypeStruct((tp_size, block, width), BF16),
        in_specs=[vmem] * 4,
        out_specs=vmem,
        scratch_shapes=[
            pltpu.VMEM((rows + 32, width), F32),
            pltpu.VMEM((rows, width), F32),
            pltpu.VMEM((rows // 128, 128), F32),
            pltpu.VMEM((tp_size, block, width), BF16),
            pltpu.VMEM((8, 128), jnp.int32),
            pltpu.VMEM((taps, 8, width), F32),
            pltpu.SemaphoreType.DMA((tp_size,)),
            pltpu.SemaphoreType.DMA((tp_size,)),
            pltpu.SemaphoreType.DMA((2,)),
            pltpu.SemaphoreType.DMA((2,)),
        ],
        compiler_params=pltpu.CompilerParams(collective_id=0, has_side_effects=True),
        cost_estimate=pl.CostEstimate(flops=30_000_000_000, bytes_accessed=4_000_000, transcendentals=0),
    )(conv_value, conv_gate, doc_ids.reshape(rows // 128, 128), conv_kernel_taps)


def project_rows(activated_rows, proj_weight):
    return jnp.dot(
        activated_rows,
        lax.all_gather(proj_weight, "tp", axis=0, tiled=True),
        preferred_element_type=jnp.float32,
    )


def body(
    mesh,
    conv_value,
    conv_gate,
    doc_ids,
    conv_kernel,
    norm_gain_conv,
    norm_bias_conv,
    proj_weight,
    residual,
    norm_gain_moe,
    group_router,
    expert_router,
    routing,
    expert_gate_w,
    expert_up_w,
    expert_down_w,
):
    raw = conv_exchange(mesh, conv_value, conv_gate, doc_ids, conv_kernel)
    raw_rows = raw.transpose(1, 0, 2).reshape(raw.shape[1], -1)
    raw_values = raw_rows.astype(jnp.float32)
    average = jnp.mean(raw_values, axis=1, keepdims=True)
    centered = raw_values - average
    variance = jnp.mean(centered * centered, axis=1, keepdims=True)
    moved_rows = jax.nn.silu(
        centered * lax.rsqrt(variance + epsilon) * norm_gain_conv + norm_bias_conv
    ).astype(jnp.bfloat16)
    projected = project_rows(moved_rows, proj_weight)
    state_values = residual.astype(jnp.float32) + projected
    hidden_state = state_values.astype(jnp.bfloat16)
    state_values = hidden_state.astype(jnp.float32)
    normed = (
        state_values
        * lax.rsqrt(jnp.mean(state_values * state_values, axis=1, keepdims=True) + epsilon)
        * norm_gain_moe
    ).astype(jnp.bfloat16)
    group_logits = jnp.dot(normed, group_router, preferred_element_type=jnp.float32)
    expert_logits = jnp.dot(normed, expert_router, preferred_element_type=jnp.float32)
    group_total = group_router.shape[1]
    expert_total = expert_router.shape[1]
    per_group = expert_total // group_total
    first_choice = routing[:, 0]
    second_choice = routing[:, 1]
    chosen_group = first_choice // per_group
    group_exp = jnp.exp(group_logits)
    group_match = chosen_group[:, None] == jnp.arange(group_total, dtype=jnp.int32)[None, :]
    group_prob = jnp.sum(jnp.where(group_match, group_exp, jnp.float32(0.0)), axis=1) / jnp.sum(
        group_exp, axis=1
    )
    expert_iota = jnp.arange(expert_total, dtype=jnp.int32)[None, :]
    first_logit = jnp.sum(
        jnp.where(first_choice[:, None] == expert_iota, expert_logits, jnp.float32(0.0)), axis=1
    )
    second_logit = jnp.sum(
        jnp.where(second_choice[:, None] == expert_iota, expert_logits, jnp.float32(0.0)), axis=1
    )
    first_exp = jnp.exp(first_logit)
    second_exp = jnp.exp(second_logit)
    first_weight = group_prob * first_exp / (first_exp + second_exp)
    second_weight = group_prob * second_exp / (first_exp + second_exp)
    row_count = normed.shape[0]
    capacity = 2 * row_count // expert_total
    flat_experts = routing.reshape(-1)
    indicator = (flat_experts[:, None] == expert_iota).astype(jnp.int32)
    before = jnp.cumsum(indicator, axis=0) - indicator
    position = jnp.sum(before * indicator, axis=1)
    destination = flat_experts * capacity + position
    source = (
        jnp.zeros((2 * row_count,), jnp.int32)
        .at[destination]
        .set(jnp.arange(2 * row_count, dtype=jnp.int32) // 2)
    )
    outgoing = normed[source].reshape(expert_total, capacity, normed.shape[1])
    arrived = lax.all_to_all(outgoing, "sp", split_axis=0, concat_axis=0, tiled=True)
    senders, slot_count, features = arrived.shape
    flattened = arrived.reshape(senders * slot_count, features)
    gate_part = jnp.dot(flattened, expert_gate_w[0], preferred_element_type=jnp.float32)
    up_part = jnp.dot(flattened, expert_up_w[0], preferred_element_type=jnp.float32)
    expert_hidden = (jax.nn.silu(gate_part) * up_part).astype(jnp.bfloat16)
    expert_result = jnp.dot(
        expert_hidden, expert_down_w[0], preferred_element_type=jnp.float32
    ).astype(jnp.bfloat16)
    returned = lax.all_to_all(
        expert_result.reshape(senders, slot_count, features),
        "sp",
        split_axis=0,
        concat_axis=0,
        tiled=True,
    )
    picked = (
        returned.reshape(2 * row_count, normed.shape[1])[destination]
        .reshape(row_count, 2, normed.shape[1])
        .astype(jnp.float32)
    )
    mixture = first_weight[:, None] * picked[:, 0] + second_weight[:, None] * picked[:, 1]
    return (state_values + mixture).astype(jnp.bfloat16)


def solution(mesh):
    placed = (
        P("sp", "tp"),
        P("sp", "tp"),
        P("sp"),
        P(None, "tp"),
        P(),
        P(),
        P("tp", None),
        P(("sp", "tp"), None),
        P(),
        P(),
        P(),
        P(("sp", "tp"), None),
        P("sp", None, None),
        P("sp", None, None),
        P("sp", None, None),
    )
    return jax.shard_map(
        functools.partial(body, mesh), mesh=mesh, in_specs=placed, out_specs=P(("sp", "tp"), None), check_vma=False
    )
```

```python
import functools
import jax
import jax.numpy as jnp
from jax import lax
from jax.experimental import pallas as pl
from jax.experimental.pallas import tpu as pltpu
from jax.sharding import PartitionSpec as P

epsilon = 1e-06
MESH = pl.DeviceIdType.MESH
F32 = jnp.float32
BF16 = jnp.bfloat16


def conv_kernel(
    sp_size, tp_size, value_ref, gate_ref, ids_ref, taps_ref, raw_ref,
    gated, reach, compact, outgoing, halo_ids, taps_wide,
    send_sem, recv_sem, halo_send, halo_recv,
):
    s = lax.axis_index("sp")
    t = lax.axis_index("tp")
    planes = tp_size // 2
    z, core = t // 2, t % 2
    rows, width = value_ref.shape
    block = rows // tp_size
    taps = taps_ref.shape[0]
    after, before = (s + 1) % sp_size, (s + sp_size - 1) % sp_size

    barrier = pltpu.get_barrier_semaphore()

    def greet(i, carry):
        other = (t + 1 + i) % tp_size
        pl.semaphore_signal(barrier, inc=1, device_id=(s, other), device_id_type=MESH)
        return carry

    lax.fori_loop(0, tp_size - 1, greet, 0)
    pl.semaphore_signal(barrier, inc=1, device_id=(after, t), device_id_type=MESH)
    pl.semaphore_signal(barrier, inc=1, device_id=(before, t), device_id_type=MESH)

    def gate_rows(r, carry):
        at = pl.multiple_of(r * 128, 128)
        v = value_ref[pl.ds(at, 128), :].astype(F32)
        g = gate_ref[pl.ds(at, 128), :].astype(F32)
        gated[pl.ds(at + 32, 128), :] = (v * jax.nn.sigmoid(g)).astype(BF16).astype(F32)
        return carry

    chunks = rows // 128
    gate_rows(chunks - 1, 0)
    wide = taps_ref[...].astype(F32)
    for k in range(taps):
        taps_wide[k] = jnp.broadcast_to(wide[k : k + 1, :], (8, width))
    pl.semaphore_wait(barrier, tp_size + 1)
    halo = pltpu.make_async_remote_copy(
        src_ref=gated.at[pl.ds(rows, 32)], dst_ref=gated.at[pl.ds(0, 32)],
        send_sem=halo_send.at[0], recv_sem=halo_recv.at[0],
        device_id=(after, t), device_id_type=MESH,
    )
    halo.start()
    halo_id = pltpu.make_async_remote_copy(
        src_ref=ids_ref.at[pl.ds(chunks - 8, 8)], dst_ref=halo_ids,
        send_sem=halo_send.at[1], recv_sem=halo_recv.at[1],
        device_id=(after, t), device_id_type=MESH,
    )
    halo_id.start()
    lax.fori_loop(0, chunks - 1, gate_rows, 0)

    ids = ids_ref[...]
    lane = lax.broadcasted_iota(jnp.int32, (chunks, 128), 1)
    row = lax.broadcasted_iota(jnp.int32, (chunks, 128), 0)
    position = row * 128 + lane
    began = jnp.zeros((chunks, 128), jnp.int32)
    for d in range(1, 16):
        count = jnp.sum(
            jnp.sum((ids < d).astype(jnp.int32), axis=1, keepdims=True), axis=0, keepdims=True
        )
        began = jnp.where(ids == d, count, began)
    halo_id.wait()
    tail_lane = lax.broadcasted_iota(jnp.int32, (1, 128), 1)
    shared = (halo_ids[7:8, :] == ids[0:1, 0:1]) & (tail_lane >= 128 - (taps - 1))
    extra = jnp.sum(shared.astype(jnp.int32), axis=1, keepdims=True)
    extra = extra * (s > 0).astype(jnp.int32)
    distance = position - began + jnp.where(began == 0, extra, 0)
    compact[...] = jnp.minimum(distance, taps).astype(F32)
    eye = (
        lax.broadcasted_iota(jnp.int32, (128, 128), 0)
        == lax.broadcasted_iota(jnp.int32, (128, 128), 1)
    ).astype(F32)
    ones = jnp.ones((128, 128), BF16)

    def widen(r, carry):
        spread = (eye * compact[pl.ds(r, 1), :]).astype(BF16)
        reach[pl.ds(pl.multiple_of(r * 128, 128), 128), :] = jnp.dot(
            spread, ones, preferred_element_type=F32
        )
        return carry

    lax.fori_loop(0, chunks, widen, 0)
    halo.wait()

    tile = 32

    def conv_block(b, store):
        def conv_tile(q, carry):
            base = pl.multiple_of(b * block + q * tile, tile)
            limit = reach[pl.ds(base, tile), :].reshape(tile // 8, 8, width)
            total = jnp.zeros((tile // 8, 8, width), F32)
            for k in range(taps):
                j = taps - 1 - k
                x = gated[pl.ds(base + (32 - j), tile), :].reshape(tile // 8, 8, width)
                total = total + jnp.where(limit >= j, x * taps_wide[k][None], 0.0)
            store(pl.multiple_of(q * tile, tile), total.reshape(tile, width).astype(BF16))
            return carry

        lax.fori_loop(0, block // tile, conv_tile, 0)

    def target(i):
        k = i // 2
        size = planes // 2 - (k + 1) // 2
        hop = (k % 2) * size + (1 - k % 2) * (planes - size)
        return ((z + hop) % planes) * 2 + (core + 1 + i) % 2

    def exchange(i):
        to = target(i)
        return pltpu.make_async_remote_copy(
            src_ref=outgoing.at[to], dst_ref=raw_ref.at[t],
            send_sem=send_sem.at[i], recv_sem=recv_sem.at[t],
            device_id=(s, to), device_id_type=MESH,
        )

    def step(i, carry):
        b = target(i)

        def store(at, value):
            outgoing[b, pl.ds(at, tile), :] = value

        conv_block(b, store)

        @pl.when(i > 0)
        def _():
            exchange(i - 1).start()

        return carry

    lax.fori_loop(0, tp_size - 1, step, 0)

    def store_own(at, value):
        raw_ref[t, pl.ds(at, tile), :] = value

    conv_block(t, store_own)
    exchange(tp_size - 2).start()

    def finish(i, carry):
        exchange(i).wait_send()
        source = (t + 1 + i) % tp_size
        pltpu.make_async_remote_copy(
            src_ref=outgoing.at[source], dst_ref=raw_ref.at[source],
            send_sem=send_sem.at[i], recv_sem=recv_sem.at[source],
            device_id=(s, source), device_id_type=MESH,
        ).wait_recv()
        return carry

    lax.fori_loop(0, tp_size - 1, finish, 0)


def conv_exchange(mesh, conv_value, conv_gate, doc_ids, conv_kernel_taps):
    sp_size, tp_size = mesh.shape["sp"], mesh.shape["tp"]
    rows, width = conv_value.shape
    block = rows // tp_size
    taps = conv_kernel_taps.shape[0]
    vmem = pl.BlockSpec(memory_space=pltpu.VMEM)
    return pl.pallas_call(
        functools.partial(conv_kernel, sp_size, tp_size),
        out_shape=jax.ShapeDtypeStruct((tp_size, block, width), BF16),
        in_specs=[vmem] * 4,
        out_specs=vmem,
        scratch_shapes=[
            pltpu.VMEM((rows + 32, width), F32),
            pltpu.VMEM((rows, width), F32),
            pltpu.VMEM((rows // 128, 128), F32),
            pltpu.VMEM((tp_size, block, width), BF16),
            pltpu.VMEM((8, 128), jnp.int32),
            pltpu.VMEM((taps, 8, width), F32),
            pltpu.SemaphoreType.DMA((tp_size,)),
            pltpu.SemaphoreType.DMA((tp_size,)),
            pltpu.SemaphoreType.DMA((2,)),
            pltpu.SemaphoreType.DMA((2,)),
        ],
        compiler_params=pltpu.CompilerParams(collective_id=0, has_side_effects=True),
        cost_estimate=pl.CostEstimate(flops=30_000_000_000, bytes_accessed=4_000_000, transcendentals=0),
    )(conv_value, conv_gate, doc_ids.reshape(rows // 128, 128), conv_kernel_taps)


def route_kernel(
    sp_size, raw_ref, weight_ref, residual_ref, gain_ref, bias_ref, moe_gain_ref,
    group_router_ref, expert_router_ref, routing_ref, routed_ref,
    gate_hbm, up_hbm, down_hbm, out_ref,
    weight, gate_w, up_w, down_w, activated, hidden, normed, squares,
    outgoing, arrived, results, returned,
    weight_sem, expert_sem, send_sem, recv_sem, back_send, back_recv,
):
    s = lax.axis_index("sp")
    t = lax.axis_index("tp")
    side = 4
    y, x = s // side, s % side
    blocks, rows, width = raw_ref.shape
    features = blocks * width
    half = features // 2
    slots = outgoing.shape[1] // 2

    barrier = pltpu.get_barrier_semaphore()
    for i in range(1, sp_size):
        pl.semaphore_signal(
            barrier, inc=1, device_id=((s + i) % sp_size, t), device_id_type=MESH
        )

    def fetch_weight(i):
        return pltpu.make_async_copy(
            weight_ref.at[pl.ds(2 * i, 2)], weight.at[pl.ds(2 * i, 2)], weight_sem.at[i]
        )

    pairs = weight.shape[0] // 2
    for i in range(pairs):
        fetch_weight(i).start()
    fetch_experts = [
        pltpu.make_async_copy(source.at[0], target, expert_sem.at[i])
        for i, (source, target) in enumerate(
            ((gate_hbm, gate_w), (up_hbm, up_w), (down_hbm, down_w))
        )
    ]
    for copy in fetch_experts:
        copy.start()

    def activate(r, carry):
        at = pl.multiple_of(r * 16, 16)
        v = raw_ref[:, pl.ds(at, 16), :].astype(F32)
        average = jnp.sum(jnp.sum(v, axis=0), axis=1, keepdims=True) * (1.0 / features)
        centered = v - average[None]
        variance = jnp.sum(jnp.sum(centered * centered, axis=0), axis=1, keepdims=True) * (
            1.0 / features
        )
        scale = lax.rsqrt(variance + epsilon)
        for b in range(blocks):
            u = centered[b] * scale * gain_ref[b : b + 1, :] + bias_ref[b : b + 1, :]
            activated[pl.ds(at, 16), b * width : (b + 1) * width] = jax.nn.silu(u).astype(BF16)
        return carry

    lax.fori_loop(0, rows // 16, activate, 0)

    experts = expert_router_ref.shape[0]
    e_lane = lax.broadcasted_iota(jnp.int32, (rows, experts), 1)
    first, second = routing_ref[:, 0:1], routing_ref[:, 1:2]
    pick_first, pick_second = first == e_lane, second == e_lane
    named = (pick_first | pick_second).astype(F32)
    lower = (
        lax.broadcasted_iota(jnp.int32, (rows, rows), 0)
        > lax.broadcasted_iota(jnp.int32, (rows, rows), 1)
    ).astype(BF16)
    earlier = jnp.dot(lower, named.astype(BF16), preferred_element_type=F32)
    first_place = first * slots + jnp.sum(
        jnp.where(pick_first, earlier, 0.0), axis=1, keepdims=True
    ).astype(jnp.int32)
    second_place = second * slots + jnp.sum(
        jnp.where(pick_second, earlier, 0.0), axis=1, keepdims=True
    ).astype(jnp.int32)

    e_row = lax.broadcasted_iota(jnp.int32, (experts, rows), 0)
    first_r, second_r = routed_ref[0:1, :], routed_ref[1:2, :]
    pick_first_r, pick_second_r = first_r == e_row, second_r == e_row
    named_r = (pick_first_r | pick_second_r).astype(F32)
    upper = (
        lax.broadcasted_iota(jnp.int32, (rows, rows), 0)
        < lax.broadcasted_iota(jnp.int32, (rows, rows), 1)
    ).astype(BF16)
    earlier_r = jnp.dot(named_r.astype(BF16), upper, preferred_element_type=F32)
    first_place_r = first_r * slots + jnp.sum(
        jnp.where(pick_first_r, earlier_r, 0.0), axis=0, keepdims=True
    ).astype(jnp.int32)
    second_place_r = second_r * slots + jnp.sum(
        jnp.where(pick_second_r, earlier_r, 0.0), axis=0, keepdims=True
    ).astype(jnp.int32)

    def expert_at(dy, dx):
        return ((y + dy) % side) * side + (x + dx) % side

    squares[...] = jnp.zeros_like(squares)

    def project(i, carry):
        fetch_weight(i).wait()
        rhs = jnp.concatenate([weight[2 * i], weight[2 * i + 1]], axis=1)
        total = jnp.dot(activated[...], rhs, preferred_element_type=F32)
        columns = pl.ds(pl.multiple_of(i * 256, 256), 256)
        state = (residual_ref[:, columns].astype(F32) + total).astype(BF16)
        hidden[:, columns] = state
        wide = state.astype(F32)
        squared = wide * wide
        squares[...] += squared[:, :128] + squared[:, 128:]
        return carry

    lax.fori_loop(0, pairs, project, 0)
    moe_scale = lax.rsqrt(
        jnp.sum(squares[...], axis=1, keepdims=True) * (1.0 / features) + epsilon
    )
    for f in range(blocks):
        columns = slice(f * width, (f + 1) * width)
        normed[:, columns] = (
            hidden[:, columns].astype(F32) * moe_scale * moe_gain_ref[f : f + 1, :]
        ).astype(BF16)

    pl.semaphore_wait(barrier, sp_size - 1)
    order = (2, 1, 3, 0)
    columns_of = (2, 1, 3, 0)

    def send(dy, dx):
        i = dy * side + dx
        return pltpu.make_async_remote_copy(
            src_ref=outgoing.at[i], dst_ref=arrived.at[i],
            send_sem=send_sem.at[i], recv_sem=recv_sem.at[i],
            device_id=(expert_at(dy, dx), t), device_id_type=MESH,
        )

    def give_back(dy, dx):
        i = dy * side + dx
        return pltpu.make_async_remote_copy(
            src_ref=results.at[i], dst_ref=returned.at[i],
            send_sem=back_send.at[i], recv_sem=back_recv.at[i],
            device_id=(expert_at(side - dy, side - dx), t), device_id_type=MESH,
        )

    def others(dy):
        return [dx for dx in columns_of if dy or dx]

    for dy in order:
        slot = lax.broadcasted_iota(jnp.int32, (side, slots, rows), 1)
        dx = lax.broadcasted_iota(jnp.int32, (side, slots, rows), 0)
        key = ((((y + dy) % side) * side) + ((x + dx) & (side - 1))) * slots + slot
        chosen = (
            ((key == first_place_r[None]) | (key == second_place_r[None]))
            .astype(F32)
            .reshape(side * slots, rows)
            .astype(BF16)
        )
        low = jnp.dot(chosen, normed[:, :half], preferred_element_type=F32)
        high = jnp.dot(chosen, normed[:, half:], preferred_element_type=F32)
        slab = jnp.concatenate(
            [low.reshape(side, slots, half), high.reshape(side, slots, half)], axis=1
        ).astype(BF16)
        if dy == 0:
            arrived[0] = slab[0]
            outgoing[1:side] = slab[1:]
        else:
            outgoing[dy * side : (dy + 1) * side] = slab
        for dx in others(dy):
            send(dy, dx).start()

    contract_last = (((1,), (1,)), ((), ()))
    group_logits = lax.dot_general(
        normed[...], group_router_ref[...], contract_last, preferred_element_type=F32
    )
    expert_logits = lax.dot_general(
        normed[...], expert_router_ref[...], contract_last, preferred_element_type=F32
    )
    groups = group_router_ref.shape[0]
    per_group = experts // groups
    group_exp = jnp.exp(group_logits)
    g_lane = lax.broadcasted_iota(jnp.int32, (rows, groups), 1)
    in_group = (first >= g_lane * per_group) & (first < (g_lane + 1) * per_group)
    group_prob = jnp.sum(jnp.where(in_group, group_exp, 0.0), axis=1, keepdims=True) / jnp.sum(
        group_exp, axis=1, keepdims=True
    )
    first_exp = jnp.exp(jnp.sum(jnp.where(pick_first, expert_logits, 0.0), axis=1, keepdims=True))
    second_exp = jnp.exp(
        jnp.sum(jnp.where(pick_second, expert_logits, 0.0), axis=1, keepdims=True)
    )
    first_weight = group_prob * first_exp / (first_exp + second_exp)
    second_weight = group_prob * second_exp / (first_exp + second_exp)

    for copy in fetch_experts:
        copy.wait()
    for dy in order:
        for dx in others(dy):
            send(dy, dx).wait()
        slab = arrived[dy * side : (dy + 1) * side].astype(F32)
        low = slab[:, :slots].reshape(side * slots, half).astype(BF16)
        high = slab[:, slots:].reshape(side * slots, half).astype(BF16)
        gated = jnp.dot(low, gate_w[:half], preferred_element_type=F32) + jnp.dot(
            high, gate_w[half:], preferred_element_type=F32
        )
        upped = jnp.dot(low, up_w[:half], preferred_element_type=F32) + jnp.dot(
            high, up_w[half:], preferred_element_type=F32
        )
        inner = (jax.nn.silu(gated) * upped).astype(BF16)
        low = jnp.dot(inner, down_w[:, :half], preferred_element_type=F32)
        high = jnp.dot(inner, down_w[:, half:], preferred_element_type=F32)
        slab = jnp.concatenate(
            [low.reshape(side, slots, half), high.reshape(side, slots, half)], axis=1
        ).astype(BF16)
        if dy == 0:
            returned[0] = slab[0]
            results[1:side] = slab[1:]
        else:
            results[dy * side : (dy + 1) * side] = slab
        for dx in others(dy):
            give_back(dy, dx).start()

    j = lax.broadcasted_iota(jnp.int32, (rows, sp_size * slots), 1)
    i = (j * 2731) >> 16
    key = (
        ((y + (i >> 2)) & (side - 1)) * side + ((x + (i & (side - 1))) & (side - 1))
    ) * slots + (j - i * slots)
    first_hot = (key == first_place).astype(BF16)
    second_hot = (key == second_place).astype(BF16)
    for dy in order:
        for dx in others(dy):
            give_back(dy, dx).wait()

    quarter = half // 4
    for h in range(2):
        for f in range(4):
            part = returned[:, h * slots : (h + 1) * slots, f * quarter : (f + 1) * quarter]
            part = part.astype(F32).reshape(sp_size * slots, quarter).astype(BF16)
            columns = slice(h * half + f * quarter, h * half + (f + 1) * quarter)
            mixed = first_weight * jnp.dot(
                first_hot, part, preferred_element_type=F32
            ) + second_weight * jnp.dot(second_hot, part, preferred_element_type=F32)
            out_ref[:, columns] = (hidden[:, columns].astype(F32) + mixed).astype(BF16)


def route(mesh, raw, weight, residual, gain, bias, moe_gain, group_router, expert_router, routing, gate_w, up_w, down_w):
    sp_size = mesh.shape["sp"]
    blocks, rows, width = raw.shape
    features = blocks * width
    slots = 2 * rows // sp_size
    inner = gate_w.shape[2]
    vmem = pl.BlockSpec(memory_space=pltpu.VMEM)
    hbm = pl.BlockSpec(memory_space=pl.ANY)
    slab = (sp_size, 2 * slots, features // 2)
    return pl.pallas_call(
        functools.partial(route_kernel, sp_size),
        out_shape=jax.ShapeDtypeStruct((rows, features), BF16),
        in_specs=[vmem, hbm, vmem, vmem, vmem, vmem, vmem, vmem, vmem, vmem, hbm, hbm, hbm],
        out_specs=vmem,
        scratch_shapes=[
            pltpu.VMEM(weight.shape, BF16),
            pltpu.VMEM((features, inner), BF16),
            pltpu.VMEM((features, inner), BF16),
            pltpu.VMEM((inner, features), BF16),
            pltpu.VMEM((rows, features), BF16),
            pltpu.VMEM((rows, features), BF16),
            pltpu.VMEM((rows, features), BF16),
            pltpu.VMEM((rows, 128), F32),
            pltpu.VMEM(slab, BF16),
            pltpu.VMEM(slab, BF16),
            pltpu.VMEM(slab, BF16),
            pltpu.VMEM(slab, BF16),
            pltpu.SemaphoreType.DMA((weight.shape[0] // 2,)),
            pltpu.SemaphoreType.DMA((3,)),
            pltpu.SemaphoreType.DMA((sp_size,)),
            pltpu.SemaphoreType.DMA((sp_size,)),
            pltpu.SemaphoreType.DMA((sp_size,)),
            pltpu.SemaphoreType.DMA((sp_size,)),
        ],
        compiler_params=pltpu.CompilerParams(collective_id=1, has_side_effects=True),
        cost_estimate=pl.CostEstimate(flops=6_000_000_000, bytes_accessed=16_000_000, transcendentals=0),
    )(
        raw, weight, residual,
        gain.reshape(blocks, width), bias.reshape(blocks, width), moe_gain.reshape(blocks, width),
        group_router.T, expert_router.T, routing, routing.T, gate_w, up_w, down_w,
    )


def body(
    mesh,
    conv_value,
    conv_gate,
    doc_ids,
    conv_kernel,
    norm_gain_conv,
    norm_bias_conv,
    proj_weight,
    residual,
    norm_gain_moe,
    group_router,
    expert_router,
    routing,
    expert_gate_w,
    expert_up_w,
    expert_down_w,
):
    part = proj_weight.shape[1] // mesh.shape["sp"]
    own = lax.dynamic_slice_in_dim(proj_weight, lax.axis_index("sp") * part, part, axis=1)
    weight = lax.all_gather(own, ("sp", "tp"), axis=0, tiled=True)
    weight = weight.reshape(mesh.shape["sp"], proj_weight.shape[1], part)
    raw = conv_exchange(mesh, conv_value, conv_gate, doc_ids, conv_kernel)
    return route(
        mesh, raw, weight, residual, norm_gain_conv, norm_bias_conv, norm_gain_moe,
        group_router, expert_router, routing, expert_gate_w, expert_up_w, expert_down_w,
    )


def solution(mesh):
    placed = (
        P("sp", "tp"),
        P("sp", "tp"),
        P("sp"),
        P(None, "tp"),
        P(),
        P(),
        P("tp", None),
        P(("sp", "tp"), None),
        P(),
        P(),
        P(),
        P(("sp", "tp"), None),
        P("sp", None, None),
        P("sp", None, None),
        P("sp", None, None),
    )
    return jax.shard_map(
        functools.partial(body, mesh), mesh=mesh, in_specs=placed, out_specs=P(("sp", "tp"), None), check_vma=False
    )
```

```python
import functools
import jax
import jax.numpy as jnp
from jax import lax
from jax.experimental import pallas as pl
from jax.experimental.pallas import tpu as pltpu
from jax.sharding import PartitionSpec as P

epsilon = 1e-06
MESH = pl.DeviceIdType.MESH
F32 = jnp.float32
BF16 = jnp.bfloat16
SIDE = 4
PAIRS = (
    ((0, 0), (0, 1)), ((0, 3), (1, 0)), ((3, 0), (1, 1)), ((1, 3), (3, 1)),
    ((3, 3), (0, 2)), ((2, 0), (1, 2)), ((2, 1), (3, 2)), ((2, 3), (2, 2)),
)


def layer_kernel(
    sp_size, tp_size,
    value_hbm, gate_hbm, ids_ref, taps_ref, gain_ref, bias_ref, proj_hbm, residual_hbm,
    moe_gain_ref, group_router_ref, expert_router_ref, routed_ref, gate_hbm_w, up_hbm_w, down_hbm_w,
    out_ref,
    value_ref, gate_ref, residual_ref, gated, reach, compact, conv_out, raw, halo_ids, taps_wide,
    own_w, far_w, gate_w, up_w, down_w, activated, hidden, normed, squares,
    outgoing, arrived, results, returned,
    local_sem, expert_sem, conv_send, conv_recv, halo_send, halo_recv,
    z_send, z_recv, a_send, a_recv, b_send, b_recv, d_send, d_recv,
    send_sem, recv_sem, back_send, back_recv,
):
    s = lax.axis_index("sp")
    t = lax.axis_index("tp")
    y, x = s // SIDE, s % SIDE
    planes = tp_size // 2
    z, core = t // 2, t % 2
    rows, width = value_ref.shape
    block = rows // tp_size
    taps = taps_ref.shape[0]
    features = tp_size * width
    half = features // 2
    slots = outgoing.shape[1] // 2
    after, before = (s + 1) % sp_size, (s + sp_size - 1) % sp_size
    chunks = rows // 128

    barrier = pltpu.get_barrier_semaphore()

    def greet(i, carry):
        pl.semaphore_signal(
            barrier, inc=1, device_id=(s, (t + 1 + i) % tp_size), device_id_type=MESH
        )
        return carry

    def greet_plane(i, carry):
        pl.semaphore_signal(
            barrier, inc=1, device_id=((s + 1 + i) % sp_size, t), device_id_type=MESH
        )
        return carry

    lax.fori_loop(0, tp_size - 1, greet, 0)
    lax.fori_loop(0, sp_size - 1, greet_plane, 0)

    head = rows - 128
    local = [
        pltpu.make_async_copy(value_hbm.at[pl.ds(head, 128)], value_ref.at[pl.ds(head, 128)], local_sem.at[0]),
        pltpu.make_async_copy(gate_hbm.at[pl.ds(head, 128)], gate_ref.at[pl.ds(head, 128)], local_sem.at[1]),
        pltpu.make_async_copy(value_hbm.at[pl.ds(0, head)], value_ref.at[pl.ds(0, head)], local_sem.at[2]),
        pltpu.make_async_copy(gate_hbm.at[pl.ds(0, head)], gate_ref.at[pl.ds(0, head)], local_sem.at[3]),
        pltpu.make_async_copy(
            proj_hbm.at[:, pl.ds(pl.multiple_of(s * width, width), width)], own_w.at[0, 0, z], local_sem.at[4]
        ),
        pltpu.make_async_copy(residual_hbm, residual_ref, local_sem.at[5]),
    ]
    for copy in local:
        copy.start()
    fetch_experts = [
        pltpu.make_async_copy(source.at[0], target, expert_sem.at[i])
        for i, (source, target) in enumerate(
            ((gate_hbm_w, gate_w), (up_hbm_w, up_w), (down_hbm_w, down_w))
        )
    ]
    for copy in fetch_experts:
        copy.start()

    ids = ids_ref[...]
    lane = lax.broadcasted_iota(jnp.int32, (chunks, 128), 1)
    row = lax.broadcasted_iota(jnp.int32, (chunks, 128), 0)
    position = row * 128 + lane
    began = jnp.zeros((chunks, 128), jnp.int32)
    for d in range(1, 16):
        count = jnp.sum(
            jnp.sum((ids < d).astype(jnp.int32), axis=1, keepdims=True), axis=0, keepdims=True
        )
        began = jnp.where(ids == d, count, began)
    compact[...] = jnp.minimum(position - began, taps).astype(F32)
    wide = taps_ref[...].astype(F32)
    for k in range(taps):
        taps_wide[k] = jnp.broadcast_to(wide[k : k + 1, :], (8, width))
    eye = (
        lax.broadcasted_iota(jnp.int32, (128, 128), 0)
        == lax.broadcasted_iota(jnp.int32, (128, 128), 1)
    ).astype(F32)
    ones = jnp.ones((128, 128), BF16)

    def widen(r, carry):
        spread = (eye * compact[pl.ds(r, 1), :]).astype(BF16)
        reach[pl.ds(pl.multiple_of(r * 128, 128), 128), :] = jnp.dot(
            spread, ones, preferred_element_type=F32
        )
        return carry

    lax.fori_loop(0, chunks, widen, 0)

    def gate_rows(r, carry):
        at = pl.multiple_of(r * 128, 128)
        v = value_ref[pl.ds(at, 128), :].astype(F32)
        g = gate_ref[pl.ds(at, 128), :].astype(F32)
        gated[pl.ds(at + 32, 128), :] = (v * jax.nn.sigmoid(g)).astype(BF16).astype(F32)
        return carry

    local[0].wait()
    local[1].wait()
    gate_rows(chunks - 1, 0)
    local[4].wait()
    pl.semaphore_wait(barrier, tp_size + sp_size - 2)

    def z_copy(h):
        return pltpu.make_async_remote_copy(
            src_ref=own_w.at[0, 0, z], dst_ref=own_w.at[0, 0, z],
            send_sem=z_send.at[h], recv_sem=z_recv.at[z],
            device_id=(s, ((z + h) % planes) * 2 + core), device_id_type=MESH,
        )

    def z_arrival(h):
        source = (z + h) % planes
        return pltpu.make_async_remote_copy(
            src_ref=own_w.at[0, 0, source], dst_ref=own_w.at[0, 0, source],
            send_sem=z_send.at[h], recv_sem=z_recv.at[source],
            device_id=(s, source * 2 + core), device_id_type=MESH,
        )

    for h in (4, 3, 5, 2, 6, 1, 7):
        z_copy(h).start()
    halo_id = pltpu.make_async_remote_copy(
        src_ref=ids_ref.at[pl.ds(chunks - 8, 8)], dst_ref=halo_ids,
        send_sem=halo_send.at[1], recv_sem=halo_recv.at[1],
        device_id=(after, t), device_id_type=MESH,
    )
    halo_id.start()
    halo = pltpu.make_async_remote_copy(
        src_ref=gated.at[pl.ds(rows, 32)], dst_ref=gated.at[pl.ds(0, 32)],
        send_sem=halo_send.at[0], recv_sem=halo_recv.at[0],
        device_id=(after, t), device_id_type=MESH,
    )
    halo.start()
    local[2].wait()
    local[3].wait()
    lax.fori_loop(0, chunks - 1, gate_rows, 0)

    halo_id.wait()
    tail_lane = lax.broadcasted_iota(jnp.int32, (1, 128), 1)
    shared = (halo_ids[7:8, :] == ids[0:1, 0:1]) & (tail_lane >= 128 - (taps - 1))
    extra = jnp.sum(shared.astype(jnp.int32), axis=1, keepdims=True)
    extra = extra * (s > 0).astype(jnp.int32)
    distance = position[0:8] - began[0:8] + jnp.where(began[0:8] == 0, extra, 0)
    compact[0:8, :] = jnp.minimum(distance, taps).astype(F32)
    widen(0, 0)
    halo.wait()

    def along_q(d):
        return (1 - core) * (y * SIDE + (x + d) % SIDE) + core * (((y + d) % SIDE) * SIDE + x)

    def along_p(d):
        return core * (y * SIDE + (x + d) % SIDE) + (1 - core) * (((y + d) % SIDE) * SIDE + x)

    lower, upper = pl.ds(0, planes // 2), pl.ds(planes // 2, planes // 2)

    def a_copy(k):
        source, target, to = (
            (own_w.at[0, 0], own_w.at[0, 3], 1),
            (own_w.at[0, 0], own_w.at[0, 1], 3),
            (own_w.at[0, 3, lower], own_w.at[0, 2, lower], 1),
            (own_w.at[0, 1, upper], own_w.at[0, 2, upper], 3),
        )[k]
        return pltpu.make_async_remote_copy(
            src_ref=source, dst_ref=target, send_sem=a_send.at[k], recv_sem=a_recv.at[k],
            device_id=(along_q(to), t), device_id_type=MESH,
        )

    def b_copy(q, k):
        source, target, to = (
            (own_w.at[0, q], own_w.at[3, q], 1),
            (own_w.at[0, q], own_w.at[1, q], 3),
            (own_w.at[3, q, lower], own_w.at[2, q, lower], 1),
            (own_w.at[1, q, upper], own_w.at[2, q, upper], 3),
        )[k]
        return pltpu.make_async_remote_copy(
            src_ref=source, dst_ref=target, send_sem=b_send.at[q, k], recv_sem=b_recv.at[q, k],
            device_id=(along_p(to), t), device_id_type=MESH,
        )

    def d_copy(p, q):
        return pltpu.make_async_remote_copy(
            src_ref=own_w.at[p, q], dst_ref=far_w.at[p, q],
            send_sem=d_send.at[p, q], recv_sem=d_recv.at[p, q],
            device_id=(s, z * 2 + 1 - core), device_id_type=MESH,
        )

    def open_gather():
        for h in (1, 7, 2, 6, 3, 5, 4):
            z_arrival(h).wait_recv()
        a_copy(0).start()
        a_copy(1).start()
        b_copy(0, 0).start()
        b_copy(0, 1).start()
        d_copy(0, 0).start()

    tile = 32

    def conv_block(b, store):
        def conv_tile(q, carry):
            base = pl.multiple_of(b * block + q * tile, tile)
            limit = reach[pl.ds(base, tile), :].reshape(tile // 8, 8, width)
            total = jnp.zeros((tile // 8, 8, width), F32)
            for k in range(taps):
                j = taps - 1 - k
                v = gated[pl.ds(base + (32 - j), tile), :].reshape(tile // 8, 8, width)
                total = total + jnp.where(limit >= j, v * taps_wide[k][None], 0.0)
            store(pl.multiple_of(q * tile, tile), total.reshape(tile, width).astype(BF16))
            return carry

        lax.fori_loop(0, block // tile, conv_tile, 0)

    def target(i):
        k = i // 2
        size = planes // 2 - (k + 1) // 2
        hop = (k % 2) * size + (1 - k % 2) * (planes - size)
        return ((z + hop) % planes) * 2 + (core + 1 + i) % 2

    def exchange(i):
        to = target(i)
        return pltpu.make_async_remote_copy(
            src_ref=conv_out.at[to], dst_ref=raw.at[t],
            send_sem=conv_send.at[i], recv_sem=conv_recv.at[t],
            device_id=(s, to), device_id_type=MESH,
        )

    def step(i, carry):
        b = target(i)

        def store(at, value):
            conv_out[b, pl.ds(at, tile), :] = value

        conv_block(b, store)

        @pl.when(i > 0)
        def _():
            exchange(i - 1).start()

        @pl.when(i == 11)
        def _():
            open_gather()

        return carry

    lax.fori_loop(0, tp_size - 1, step, 0)

    def store_own(at, value):
        raw[t, pl.ds(at, tile), :] = value

    conv_block(t, store_own)
    exchange(tp_size - 2).start()

    for k in range(2):
        a_copy(k).wait_recv()
    for k in (2, 3):
        a_copy(k).start()
    for q in (3, 1):
        b_copy(q, 0).start()
        b_copy(q, 1).start()
        d_copy(0, q).start()

    experts = expert_router_ref.shape[0]
    e_row = lax.broadcasted_iota(jnp.int32, (experts, block), 0)
    first_r, second_r = routed_ref[0:1, :], routed_ref[1:2, :]
    pick_first_r, pick_second_r = first_r == e_row, second_r == e_row
    named_r = (pick_first_r | pick_second_r).astype(F32)
    token_r = lax.broadcasted_iota(jnp.int32, (block, block), 0)
    token_c = lax.broadcasted_iota(jnp.int32, (block, block), 1)
    earlier_r = jnp.dot(
        named_r.astype(BF16), (token_r < token_c).astype(BF16), preferred_element_type=F32
    )
    first_rank = jnp.sum(jnp.where(pick_first_r, earlier_r, 0.0), axis=0, keepdims=True)
    second_rank = jnp.sum(jnp.where(pick_second_r, earlier_r, 0.0), axis=0, keepdims=True)
    first_place_r = first_r * slots + first_rank.astype(jnp.int32)
    second_place_r = second_r * slots + second_rank.astype(jnp.int32)
    standing = jnp.concatenate(
        [
            first_r.astype(F32), second_r.astype(F32), first_rank, second_rank,
            jnp.zeros((4, block), F32),
        ],
        axis=0,
    ).astype(BF16)
    contract_last = (((1,), (1,)), ((), ()))
    turned = lax.dot_general(
        (token_r == token_c).astype(BF16), standing, contract_last, preferred_element_type=F32
    ).astype(jnp.int32)
    first, second = turned[:, 0:1], turned[:, 1:2]
    first_place = first * slots + turned[:, 2:3]
    second_place = second * slots + turned[:, 3:4]

    for k in (2, 3):
        a_copy(k).wait_recv()
    b_copy(2, 0).start()
    b_copy(2, 1).start()
    d_copy(0, 2).start()

    def relay(q):
        b_copy(q, 0).wait_recv()
        b_copy(q, 1).wait_recv()
        b_copy(q, 2).start()
        b_copy(q, 3).start()
        d_copy(3, q).start()
        d_copy(1, q).start()

    for q in (0, 3, 1):
        relay(q)

    def conv_arrival(i, carry):
        source = (t + 1 + i) % tp_size
        pltpu.make_async_remote_copy(
            src_ref=conv_out.at[source], dst_ref=raw.at[source],
            send_sem=conv_send.at[i], recv_sem=conv_recv.at[source],
            device_id=(s, source), device_id_type=MESH,
        ).wait_recv()
        return carry

    lax.fori_loop(0, tp_size - 1, conv_arrival, 0)

    def activate(r, carry):
        at = pl.multiple_of(r * 16, 16)
        v = raw[:, pl.ds(at, 16), :].astype(F32)
        average = jnp.sum(jnp.sum(v, axis=0), axis=1, keepdims=True) * (1.0 / features)
        centered = v - average[None]
        variance = jnp.sum(jnp.sum(centered * centered, axis=0), axis=1, keepdims=True) * (
            1.0 / features
        )
        scale = lax.rsqrt(variance + epsilon)
        for b in range(tp_size):
            u = centered[b] * scale * gain_ref[b : b + 1, :] + bias_ref[b : b + 1, :]
            activated[b % 2, pl.ds(at, 16), (b // 2) * width : (b // 2 + 1) * width] = (
                jax.nn.silu(u).astype(BF16)
            )
        return carry

    lax.fori_loop(0, block // 16, activate, 0)
    for q in (2,):
        relay(q)

    def expert_at(dy, dx):
        return ((y + dy) % SIDE) * SIDE + (x + dx) % SIDE

    squares[...] = jnp.zeros_like(squares)
    local[5].wait()

    def project(pair):
        def column(source, swap):
            parts = []
            for dy, dx in pair:
                i = dy * (1 - swap) + dx * swap
                k = dx * (1 - swap) + dy * swap
                parts.append(source[i, k].reshape(planes * width, width))
            return jnp.concatenate(parts, axis=1)

        total = jnp.dot(
            activated[core], column(own_w, core), preferred_element_type=F32
        ) + jnp.dot(activated[1 - core], column(far_w, 1 - core), preferred_element_type=F32)
        for n, (dy, dx) in enumerate(pair):
            columns = pl.ds(pl.multiple_of(expert_at(dy, dx) * width, width), width)
            state = (
                residual_ref[:, columns].astype(F32) + total[:, n * width : (n + 1) * width]
            ).astype(BF16)
            hidden[:, columns] = state
            wide_state = state.astype(F32)
            squares[...] += wide_state * wide_state

    near = (0, 1, 3)
    for p in near:
        for q in near:
            d_copy(p, q).wait_recv()
    for pair in PAIRS[:2]:
        project(pair)
    for q in (0, 3):
        b_copy(q, 2).wait_recv()
        b_copy(q, 3).wait_recv()
        d_copy(2, q).start()
    for pair in PAIRS[2:4]:
        project(pair)
    for q in (1, 2):
        b_copy(q, 2).wait_recv()
        b_copy(q, 3).wait_recv()
        d_copy(2, q).start()
    for p, q in ((0, 2), (1, 2), (3, 2), (2, 0), (2, 3), (2, 1), (2, 2)):
        d_copy(p, q).wait_recv()
    for pair in PAIRS[4:]:
        project(pair)

    moe_scale = lax.rsqrt(
        jnp.sum(squares[...], axis=1, keepdims=True) * (1.0 / features) + epsilon
    )
    for f in range(tp_size):
        columns = slice(f * width, (f + 1) * width)
        normed[:, columns] = (
            hidden[:, columns].astype(F32) * moe_scale * moe_gain_ref[f : f + 1, :]
        ).astype(BF16)

    order = (2, 1, 3, 0)
    columns_of = (2, 1, 3, 0)

    def send(dy, dx):
        i = dy * SIDE + dx
        return pltpu.make_async_remote_copy(
            src_ref=outgoing.at[i], dst_ref=arrived.at[i],
            send_sem=send_sem.at[i], recv_sem=recv_sem.at[i],
            device_id=(expert_at(dy, dx), t), device_id_type=MESH,
        )

    def give_back(dy, dx):
        i = dy * SIDE + dx
        return pltpu.make_async_remote_copy(
            src_ref=results.at[i], dst_ref=returned.at[i],
            send_sem=back_send.at[i], recv_sem=back_recv.at[i],
            device_id=(expert_at(SIDE - dy, SIDE - dx), t), device_id_type=MESH,
        )

    def others(dy):
        return [dx for dx in columns_of if dy or dx]

    for dy in order:
        slot = lax.broadcasted_iota(jnp.int32, (SIDE, slots, block), 1)
        dx = lax.broadcasted_iota(jnp.int32, (SIDE, slots, block), 0)
        key = ((((y + dy) % SIDE) * SIDE) + ((x + dx) & (SIDE - 1))) * slots + slot
        chosen = (
            ((key == first_place_r[None]) | (key == second_place_r[None]))
            .astype(F32)
            .reshape(SIDE * slots, block)
            .astype(BF16)
        )
        low = jnp.dot(chosen, normed[:, :half], preferred_element_type=F32)
        high = jnp.dot(chosen, normed[:, half:], preferred_element_type=F32)
        slab = jnp.concatenate(
            [low.reshape(SIDE, slots, half), high.reshape(SIDE, slots, half)], axis=1
        ).astype(BF16)
        if dy == 0:
            arrived[0] = slab[0]
            outgoing[1:SIDE] = slab[1:]
        else:
            outgoing[dy * SIDE : (dy + 1) * SIDE] = slab
        for dx in others(dy):
            send(dy, dx).start()

    group_logits = lax.dot_general(
        normed[...], group_router_ref[...], contract_last, preferred_element_type=F32
    )
    expert_logits = lax.dot_general(
        normed[...], expert_router_ref[...], contract_last, preferred_element_type=F32
    )
    e_lane = lax.broadcasted_iota(jnp.int32, (block, experts), 1)
    groups = group_router_ref.shape[0]
    per_group = experts // groups
    group_exp = jnp.exp(group_logits)
    g_lane = lax.broadcasted_iota(jnp.int32, (block, groups), 1)
    in_group = (first >= g_lane * per_group) & (first < (g_lane + 1) * per_group)
    group_prob = jnp.sum(jnp.where(in_group, group_exp, 0.0), axis=1, keepdims=True) / jnp.sum(
        group_exp, axis=1, keepdims=True
    )
    first_exp = jnp.exp(jnp.sum(jnp.where(first == e_lane, expert_logits, 0.0), axis=1, keepdims=True))
    second_exp = jnp.exp(
        jnp.sum(jnp.where(second == e_lane, expert_logits, 0.0), axis=1, keepdims=True)
    )
    first_weight = group_prob * first_exp / (first_exp + second_exp)
    second_weight = group_prob * second_exp / (first_exp + second_exp)

    for copy in fetch_experts:
        copy.wait()
    for dy in order:
        for dx in others(dy):
            send(dy, dx).wait()
        slab = arrived[dy * SIDE : (dy + 1) * SIDE].astype(F32)
        low = slab[:, :slots].reshape(SIDE * slots, half).astype(BF16)
        high = slab[:, slots:].reshape(SIDE * slots, half).astype(BF16)
        gated = jnp.dot(low, gate_w[:half], preferred_element_type=F32) + jnp.dot(
            high, gate_w[half:], preferred_element_type=F32
        )
        upped = jnp.dot(low, up_w[:half], preferred_element_type=F32) + jnp.dot(
            high, up_w[half:], preferred_element_type=F32
        )
        inner = (jax.nn.silu(gated) * upped).astype(BF16)
        low = jnp.dot(inner, down_w[:, :half], preferred_element_type=F32)
        high = jnp.dot(inner, down_w[:, half:], preferred_element_type=F32)
        slab = jnp.concatenate(
            [low.reshape(SIDE, slots, half), high.reshape(SIDE, slots, half)], axis=1
        ).astype(BF16)
        if dy == 0:
            returned[0] = slab[0]
            results[1:SIDE] = slab[1:]
        else:
            results[dy * SIDE : (dy + 1) * SIDE] = slab
        for dx in others(dy):
            give_back(dy, dx).start()

    j = lax.broadcasted_iota(jnp.int32, (block, sp_size * slots), 1)
    i = (j * 2731) >> 16
    key = (
        ((y + (i >> 2)) & (SIDE - 1)) * SIDE + ((x + (i & (SIDE - 1))) & (SIDE - 1))
    ) * slots + (j - i * slots)
    first_hot = (key == first_place).astype(BF16)
    second_hot = (key == second_place).astype(BF16)
    for dy in order:
        for dx in others(dy):
            give_back(dy, dx).wait()

    quarter = half // 4
    for h in range(2):
        for f in range(4):
            part = returned[:, h * slots : (h + 1) * slots, f * quarter : (f + 1) * quarter]
            part = part.astype(F32).reshape(sp_size * slots, quarter).astype(BF16)
            columns = slice(h * half + f * quarter, h * half + (f + 1) * quarter)
            mixed = first_weight * jnp.dot(
                first_hot, part, preferred_element_type=F32
            ) + second_weight * jnp.dot(second_hot, part, preferred_element_type=F32)
            out_ref[:, columns] = (hidden[:, columns].astype(F32) + mixed).astype(BF16)

    for i in range(tp_size - 1):
        exchange(i).wait_send()
    for h in range(1, planes):
        z_copy(h).wait_send()
    for k in range(4):
        a_copy(k).wait_send()
    for q in range(SIDE):
        for k in range(4):
            b_copy(q, k).wait_send()
    for p in range(SIDE):
        for q in range(SIDE):
            d_copy(p, q).wait_send()


def body(
    mesh, conv_value, conv_gate, doc_ids, conv_kernel, norm_gain_conv, norm_bias_conv,
    proj_weight, residual, norm_gain_moe, group_router, expert_router, routing,
    expert_gate_w, expert_up_w, expert_down_w,
):
    sp_size, tp_size = mesh.shape["sp"], mesh.shape["tp"]
    rows, width = conv_value.shape
    block = rows // tp_size
    features = tp_size * width
    taps = conv_kernel.shape[0]
    inner = expert_gate_w.shape[2]
    slots = 2 * block // sp_size
    planes = tp_size // 2
    vmem = pl.BlockSpec(memory_space=pltpu.VMEM)
    hbm = pl.BlockSpec(memory_space=pl.ANY)
    slab = (sp_size, 2 * slots, features // 2)
    dma = pltpu.SemaphoreType.DMA
    return pl.pallas_call(
        functools.partial(layer_kernel, sp_size, tp_size),
        out_shape=jax.ShapeDtypeStruct((block, features), BF16),
        in_specs=[hbm, hbm, vmem, vmem, vmem, vmem, hbm, hbm, vmem, vmem, vmem, vmem, hbm, hbm, hbm],
        out_specs=vmem,
        scratch_shapes=[
            pltpu.VMEM((rows, width), BF16),
            pltpu.VMEM((rows, width), BF16),
            pltpu.VMEM((block, features), BF16),
            pltpu.VMEM((rows + 32, width), F32),
            pltpu.VMEM((rows, width), F32),
            pltpu.VMEM((rows // 128, 128), F32),
            pltpu.VMEM((tp_size, block, width), BF16),
            pltpu.VMEM((tp_size, block, width), BF16),
            pltpu.VMEM((8, 128), jnp.int32),
            pltpu.VMEM((taps, 8, width), F32),
            pltpu.VMEM((SIDE, SIDE, planes, width, width), BF16),
            pltpu.VMEM((SIDE, SIDE, planes, width, width), BF16),
            pltpu.VMEM((features, inner), BF16),
            pltpu.VMEM((features, inner), BF16),
            pltpu.VMEM((inner, features), BF16),
            pltpu.VMEM((2, block, features // 2), BF16),
            pltpu.VMEM((block, features), BF16),
            pltpu.VMEM((block, features), BF16),
            pltpu.VMEM((block, 128), F32),
            pltpu.VMEM(slab, BF16),
            pltpu.VMEM(slab, BF16),
            pltpu.VMEM(slab, BF16),
            pltpu.VMEM(slab, BF16),
            dma((6,)), dma((3,)), dma((tp_size,)), dma((tp_size,)), dma((2,)), dma((2,)),
            dma((planes,)), dma((planes,)), dma((4,)), dma((4,)),
            dma((SIDE, 4)), dma((SIDE, 4)), dma((SIDE, SIDE)), dma((SIDE, SIDE)),
            dma((sp_size,)), dma((sp_size,)), dma((sp_size,)), dma((sp_size,)),
        ],
        compiler_params=pltpu.CompilerParams(collective_id=0, has_side_effects=True),
    )(
        conv_value, conv_gate, doc_ids.reshape(rows // 128, 128), conv_kernel,
        norm_gain_conv.reshape(tp_size, width), norm_bias_conv.reshape(tp_size, width),
        proj_weight, residual, norm_gain_moe.reshape(tp_size, width),
        group_router.T, expert_router.T, routing.T, expert_gate_w, expert_up_w, expert_down_w,
    )


def solution(mesh):
    placed = (
        P("sp", "tp"),
        P("sp", "tp"),
        P("sp"),
        P(None, "tp"),
        P(),
        P(),
        P("tp", None),
        P(("sp", "tp"), None),
        P(),
        P(),
        P(),
        P(("sp", "tp"), None),
        P("sp", None, None),
        P("sp", None, None),
        P("sp", None, None),
    )
    return jax.shard_map(
        functools.partial(body, mesh), mesh=mesh, in_specs=placed, out_specs=P(("sp", "tp"), None), check_vma=False
    )
```

```python
import functools
import jax
import jax.numpy as jnp
from jax import lax
from jax.experimental import pallas as pl
from jax.experimental.pallas import tpu as pltpu
from jax.sharding import PartitionSpec as P

epsilon = 1e-06
MESH = pl.DeviceIdType.MESH
F32 = jnp.float32
BF16 = jnp.bfloat16
SIDE = 4
HOPS = (0, 1, 7, 2, 6, 3, 5, 4)
PIECES = ((1, 2), (3, 2), (5, 3))
PAIRS = (
    ((0, 0), (0, 1)), ((0, 3), (1, 0)), ((3, 0), (1, 1)), ((1, 3), (3, 1)),
    ((3, 3), (0, 2)), ((2, 0), (1, 2)), ((2, 1), (3, 2)), ((2, 3), (2, 2)),
)


def layer_kernel(
    sp_size, tp_size,
    value_hbm, gate_hbm, ids_ref, taps_ref, gain_ref, bias_ref, proj_hbm, residual_hbm,
    moe_gain_ref, group_router_ref, expert_router_ref, routed_ref, gate_hbm_w, up_hbm_w, down_hbm_w,
    out_ref,
    value_ref, gate_ref, residual_ref, gated, reach, compact, conv_out, raw, halo_ids, taps_wide,
    first_w, own_w, far_w, gate_w, up_w, down_w, activated, hidden, normed, squares,
    outgoing, arrived, results, returned,
    local_sem, rows_sem, expert_sem, conv_send, conv_recv, halo_send, halo_recv,
    z_send, z_recv, a_send, a_recv, b_send, b_recv, d_send, d_recv,
    send_sem, recv_sem, back_send, back_recv,
):
    s = lax.axis_index("sp")
    t = lax.axis_index("tp")
    y, x = s // SIDE, s % SIDE
    planes = tp_size // 2
    z, core = t // 2, t % 2
    rows, width = value_ref.shape
    block = rows // tp_size
    taps = taps_ref.shape[0]
    features = tp_size * width
    half = features // 2
    slots = outgoing.shape[1] // 2
    after, before = (s + 1) % sp_size, (s + sp_size - 1) % sp_size
    chunks = rows // 128

    barrier = pltpu.get_barrier_semaphore()

    def greet(i, carry):
        pl.semaphore_signal(
            barrier, inc=1, device_id=(s, (t + 1 + i) % tp_size), device_id_type=MESH
        )
        return carry

    def greet_plane(i, carry):
        pl.semaphore_signal(
            barrier, inc=1, device_id=((s + 1 + i) % sp_size, t), device_id_type=MESH
        )
        return carry

    lax.fori_loop(0, tp_size - 1, greet, 0)
    lax.fori_loop(0, sp_size - 1, greet_plane, 0)

    def expert_at(dy, dx):
        return ((y + dy) % SIDE) * SIDE + (x + dx) % SIDE

    def block_at(p, q):
        dy = (1 - core) * p + core * q
        dx = (1 - core) * q + core * p
        return expert_at(dy, dx)

    head = rows - 128
    local = [
        pltpu.make_async_copy(value_hbm.at[pl.ds(head, 128)], value_ref.at[pl.ds(head, 128)], local_sem.at[0]),
        pltpu.make_async_copy(gate_hbm.at[pl.ds(head, 128)], gate_ref.at[pl.ds(head, 128)], local_sem.at[1]),
        pltpu.make_async_copy(
            proj_hbm.at[:, pl.ds(pl.multiple_of(s * width, width), width)], first_w, local_sem.at[2]
        ),
        pltpu.make_async_copy(value_hbm.at[pl.ds(0, head)], value_ref.at[pl.ds(0, head)], local_sem.at[3]),
        pltpu.make_async_copy(gate_hbm.at[pl.ds(0, head)], gate_ref.at[pl.ds(0, head)], local_sem.at[4]),
        pltpu.make_async_copy(residual_hbm, residual_ref, local_sem.at[5]),
    ]
    for copy in local:
        copy.start()

    def own_rows(p, q):
        return pltpu.make_async_copy(
            proj_hbm.at[:, pl.ds(pl.multiple_of(block_at(p, q) * width, width), width)],
            own_w.at[p, q, 0], rows_sem.at[p, q],
        )

    for p in range(SIDE):
        for q in range(SIDE):
            own_rows(p, q).start()
    fetch_experts = [
        pltpu.make_async_copy(source.at[0], target, expert_sem.at[i])
        for i, (source, target) in enumerate(
            ((gate_hbm_w, gate_w), (up_hbm_w, up_w), (down_hbm_w, down_w))
        )
    ]
    for copy in fetch_experts:
        copy.start()

    def gate_rows(at, size):
        v = value_ref[pl.ds(at, size), :].astype(F32)
        g = gate_ref[pl.ds(at, size), :].astype(F32)
        gated[pl.ds(at + 32, size), :] = (v * jax.nn.sigmoid(g)).astype(BF16).astype(F32)

    local[0].wait()
    local[1].wait()
    gate_rows(head, 128)

    ids = ids_ref[...]
    lane = lax.broadcasted_iota(jnp.int32, (chunks, 128), 1)
    row = lax.broadcasted_iota(jnp.int32, (chunks, 128), 0)
    position = row * 128 + lane
    ones = jnp.ones((128, 128), BF16)
    below = jnp.concatenate(
        [jnp.sum((ids < d).astype(F32), axis=0, keepdims=True) for d in range(16)], axis=0
    )
    counts = jnp.dot(below.astype(BF16), ones, preferred_element_type=F32).astype(jnp.int32)
    began = jnp.zeros((chunks, 128), jnp.int32)
    for d in range(1, 16):
        began = jnp.where(ids == d, counts[d : d + 1, :], began)
    compact[...] = jnp.minimum(position - began, taps).astype(F32)
    eye = (
        lax.broadcasted_iota(jnp.int32, (128, 128), 0)
        == lax.broadcasted_iota(jnp.int32, (128, 128), 1)
    ).astype(F32)

    def widen(r, size):
        spread = [(eye * compact[pl.ds(r + n, 1), :]).astype(BF16) for n in range(size)]
        reach[pl.ds(pl.multiple_of(r * 128, 128), 128 * size), :] = jnp.dot(
            jnp.concatenate(spread, axis=0), ones, preferred_element_type=F32
        )

    def z_copy(h):
        return pltpu.make_async_remote_copy(
            src_ref=first_w, dst_ref=own_w.at[0, 0, HOPS.index(planes - h)],
            send_sem=z_send.at[h], recv_sem=z_recv.at[planes - h],
            device_id=(s, ((z + h) % planes) * 2 + core), device_id_type=MESH,
        )

    def z_arrival(h):
        return pltpu.make_async_remote_copy(
            src_ref=first_w, dst_ref=own_w.at[0, 0, HOPS.index(h)],
            send_sem=z_send.at[h], recv_sem=z_recv.at[h],
            device_id=(s, ((z + h) % planes) * 2 + core), device_id_type=MESH,
        )

    local[2].wait()
    pl.semaphore_wait(barrier, tp_size + sp_size - 2)
    for h in HOPS[1:]:
        z_copy(h).start()
    halo_id = pltpu.make_async_remote_copy(
        src_ref=ids_ref.at[pl.ds(chunks - 8, 8)], dst_ref=halo_ids,
        send_sem=halo_send.at[1], recv_sem=halo_recv.at[1],
        device_id=(after, t), device_id_type=MESH,
    )
    halo_id.start()
    halo = pltpu.make_async_remote_copy(
        src_ref=gated.at[pl.ds(rows, 32)], dst_ref=gated.at[pl.ds(0, 32)],
        send_sem=halo_send.at[0], recv_sem=halo_recv.at[0],
        device_id=(after, t), device_id_type=MESH,
    )
    halo.start()

    def widen_step(r, carry):
        widen(r * 8, 8)
        return carry

    lax.fori_loop(0, chunks // 8, widen_step, 0)
    wide = taps_ref[...].astype(F32)
    for k in range(taps):
        taps_wide[k] = jnp.broadcast_to(wide[k : k + 1, :], (8, width))
    local[3].wait()
    local[4].wait()
    gate_rows(head - 256, 256)

    def gate_step(r, carry):
        gate_rows(pl.multiple_of(r * 384, 128), 384)
        return carry

    lax.fori_loop(0, (head - 256) // 384, gate_step, 0)

    def receive_halo():
        halo_id.wait()
        tail_lane = lax.broadcasted_iota(jnp.int32, (1, 128), 1)
        shared = (halo_ids[7:8, :] == ids_ref[0:1, 0:1]) & (tail_lane >= 128 - (taps - 1))
        extra = jnp.sum(shared.astype(F32), axis=1, keepdims=True)
        extra = extra * (s > 0).astype(F32)
        place = lax.broadcasted_iota(jnp.int32, (1, 128), 1).astype(F32)
        near = compact[0:1, :]
        joined = (near == place).astype(F32)
        compact[0:1, :] = jnp.minimum(near + joined * extra, float(taps))
        widen(0, 1)
        halo.wait()

    def along_q(d):
        return (1 - core) * (y * SIDE + (x + d) % SIDE) + core * (((y + d) % SIDE) * SIDE + x)

    def along_p(d):
        return core * (y * SIDE + (x + d) % SIDE) + (1 - core) * (((y + d) % SIDE) * SIDE + x)

    rest, lower, upper = pl.ds(1, 7), pl.ds(1, 4), pl.ds(5, 3)

    def remote(source, target, send, recv, to):
        return pltpu.make_async_remote_copy(
            src_ref=source, dst_ref=target, send_sem=send, recv_sem=recv,
            device_id=(to, t), device_id_type=MESH,
        )

    def a_copy(k, n=0):
        cut = pl.ds(*PIECES[n]) if k < 2 else (lower, upper)[k - 2]
        origin, landing, to = ((0, 3, 1), (0, 1, 3), (3, 2, 1), (1, 2, 3))[k]
        return remote(
            own_w.at[0, origin, cut], own_w.at[0, landing, cut],
            a_send.at[k, n], a_recv.at[k, n], along_q(to),
        )

    def b_copy(q, k, n=0):
        cut = (pl.ds(*PIECES[n]) if q == 0 else rest) if k < 2 else (lower, upper)[k - 2]
        origin, landing, to = ((0, 3, 1), (0, 1, 3), (3, 2, 1), (1, 2, 3))[k]
        return remote(
            own_w.at[origin, q, cut], own_w.at[landing, q, cut],
            b_send.at[q, k, n], b_recv.at[q, k, n], along_p(to),
        )

    def pieces_of(q, k):
        return len(PIECES) if k < 2 and q == 0 else 1

    def d_copy(p, q):
        return pltpu.make_async_remote_copy(
            src_ref=own_w.at[p, q], dst_ref=far_w.at[p, q],
            send_sem=d_send.at[p, q], recv_sem=d_recv.at[p, q],
            device_id=(s, z * 2 + 1 - core), device_id_type=MESH,
        )

    def open_gather(n):
        for m in range(PIECES[n][0], PIECES[n][0] + PIECES[n][1]):
            z_arrival(HOPS[m]).wait_recv()
        a_copy(0, n).start()
        a_copy(1, n).start()
        b_copy(0, 0, n).start()
        b_copy(0, 1, n).start()
        if n == len(PIECES) - 1:
            own_rows(0, 0).wait()
            d_copy(0, 0).start()

    tile = 32

    def conv_block(b, store):
        def conv_tile(q, carry):
            base = pl.multiple_of(b * block + q * tile, tile)
            limit = reach[pl.ds(base, tile), :].reshape(tile // 8, 8, width)
            total = jnp.zeros((tile // 8, 8, width), F32)
            for k in range(taps):
                j = taps - 1 - k
                v = gated[pl.ds(base + (32 - j), tile), :].reshape(tile // 8, 8, width)
                total = total + jnp.where(limit >= j, v * taps_wide[k][None], 0.0)
            store(pl.multiple_of(q * tile, tile), total.reshape(tile, width).astype(BF16))
            return carry

        lax.fori_loop(0, block // tile, conv_tile, 0)

    def rank(i):
        k = i // 2
        size = planes // 2 - (k + 1) // 2
        hop = (k % 2) * size + (1 - k % 2) * (planes - size)
        return ((z + hop) % planes) * 2 + (core + 1 + i) % 2

    early = rank(14)
    met = sum((rank(i) == 0).astype(jnp.int32) for i in range(14))

    def flag(truth):
        return int(truth) if isinstance(truth, bool) else truth.astype(jnp.int32)

    def target(i):
        to = rank(i)
        first = (to == 0).astype(jnp.int32) * flag(i < 14)
        swap = flag(i == 14)
        return (to + first * early) * (1 - swap * met)

    def exchange(i):
        to = target(i)
        return pltpu.make_async_remote_copy(
            src_ref=conv_out.at[to], dst_ref=raw.at[t],
            send_sem=conv_send.at[i], recv_sem=conv_recv.at[t],
            device_id=(s, to), device_id_type=MESH,
        )

    def step(i, carry):
        b = target(i)

        @pl.when(i == 14)
        def _():
            receive_halo()

        def store(at, value):
            conv_out[b, pl.ds(at, tile), :] = value

        conv_block(b, store)

        @pl.when(i > 0)
        def _():
            exchange(i - 1).start()

        for n, at in enumerate((4, 8, 12)):

            @pl.when(i == at)
            def _(n=n):
                open_gather(n)

        return carry

    lax.fori_loop(0, tp_size - 1, step, 0)

    def store_own(at, value):
        raw[t, pl.ds(at, tile), :] = value

    conv_block(t, store_own)
    exchange(tp_size - 2).start()

    for k in range(2):
        for n in range(len(PIECES)):
            a_copy(k, n).wait_recv()
    for k in (2, 3):
        a_copy(k).start()
    for q in (3, 1):
        b_copy(q, 0).start()
        b_copy(q, 1).start()
        own_rows(0, q).wait()
        d_copy(0, q).start()

    experts = expert_router_ref.shape[0]
    e_row = lax.broadcasted_iota(jnp.int32, (experts, block), 0)
    first_r, second_r = routed_ref[0:1, :], routed_ref[1:2, :]
    pick_first_r, pick_second_r = first_r == e_row, second_r == e_row
    named_r = (pick_first_r | pick_second_r).astype(F32)
    token_r = lax.broadcasted_iota(jnp.int32, (block, block), 0)
    token_c = lax.broadcasted_iota(jnp.int32, (block, block), 1)
    earlier_r = jnp.dot(
        named_r.astype(BF16), (token_r < token_c).astype(BF16), preferred_element_type=F32
    )
    first_rank = jnp.sum(jnp.where(pick_first_r, earlier_r, 0.0), axis=0, keepdims=True)
    second_rank = jnp.sum(jnp.where(pick_second_r, earlier_r, 0.0), axis=0, keepdims=True)
    first_place_r = first_r * slots + first_rank.astype(jnp.int32)
    second_place_r = second_r * slots + second_rank.astype(jnp.int32)
    standing = jnp.concatenate(
        [
            first_r.astype(F32), second_r.astype(F32), first_rank, second_rank,
            jnp.zeros((4, block), F32),
        ],
        axis=0,
    ).astype(BF16)
    contract_last = (((1,), (1,)), ((), ()))
    turned = lax.dot_general(
        (token_r == token_c).astype(BF16), standing, contract_last, preferred_element_type=F32
    ).astype(jnp.int32)
    first, second = turned[:, 0:1], turned[:, 1:2]
    first_place = first * slots + turned[:, 2:3]
    second_place = second * slots + turned[:, 3:4]

    for k in (2, 3):
        a_copy(k).wait_recv()
    b_copy(2, 0).start()
    b_copy(2, 1).start()
    own_rows(0, 2).wait()
    d_copy(0, 2).start()

    def relay(q):
        for k in range(2):
            for n in range(pieces_of(q, k)):
                b_copy(q, k, n).wait_recv()
        b_copy(q, 2).start()
        b_copy(q, 3).start()
        for p in (3, 1):
            own_rows(p, q).wait()
            d_copy(p, q).start()

    def close(q):
        b_copy(q, 2).wait_recv()
        b_copy(q, 3).wait_recv()
        own_rows(2, q).wait()
        d_copy(2, q).start()

    for q in (0, 3, 1):
        relay(q)

    def conv_arrival(i, carry):
        source = (t + 1 + i) % tp_size
        pltpu.make_async_remote_copy(
            src_ref=conv_out.at[source], dst_ref=raw.at[source],
            send_sem=conv_send.at[i], recv_sem=conv_recv.at[source],
            device_id=(s, source), device_id_type=MESH,
        ).wait_recv()
        return carry

    lax.fori_loop(0, tp_size - 1, conv_arrival, 0)

    def activate(r, carry):
        at = pl.multiple_of(r * 16, 16)
        v = raw[:, pl.ds(at, 16), :].astype(F32)
        average = jnp.sum(jnp.sum(v, axis=0), axis=1, keepdims=True) * (1.0 / features)
        centered = v - average[None]
        variance = jnp.sum(jnp.sum(centered * centered, axis=0), axis=1, keepdims=True) * (
            1.0 / features
        )
        scale = lax.rsqrt(variance + epsilon)
        for m in range(planes):
            for side in range(2):
                b = ((z + HOPS[m]) % planes) * 2 + side
                u = raw[b, pl.ds(at, 16), :].astype(F32) - average
                u = u * scale * gain_ref[pl.ds(b, 1), :] + bias_ref[pl.ds(b, 1), :]
                activated[side, pl.ds(at, 16), m * width : (m + 1) * width] = (
                    jax.nn.silu(u).astype(BF16)
                )
        return carry

    lax.fori_loop(0, block // 16, activate, 0)
    for q in (2,):
        relay(q)

    squares[...] = jnp.zeros_like(squares)
    local[5].wait()

    def project(pair):
        def column(source, swap):
            parts = []
            for dy, dx in pair:
                i = dy * (1 - swap) + dx * swap
                k = dx * (1 - swap) + dy * swap
                parts.append(source[i, k].reshape(planes * width, width))
            return jnp.concatenate(parts, axis=1)

        total = jnp.dot(
            activated[core], column(own_w, core), preferred_element_type=F32
        ) + jnp.dot(activated[1 - core], column(far_w, 1 - core), preferred_element_type=F32)
        for n, (dy, dx) in enumerate(pair):
            columns = pl.ds(pl.multiple_of(expert_at(dy, dx) * width, width), width)
            state = (
                residual_ref[:, columns].astype(F32) + total[:, n * width : (n + 1) * width]
            ).astype(BF16)
            hidden[:, columns] = state
            wide_state = state.astype(F32)
            squares[...] += wide_state * wide_state

    near = (0, 1, 3)
    for p in near:
        for q in near:
            d_copy(p, q).wait_recv()
    for pair in PAIRS[:2]:
        project(pair)
    for q in (0, 3):
        close(q)
    for pair in PAIRS[2:4]:
        project(pair)
    for q in (1, 2):
        close(q)
    for p, q in ((0, 2), (1, 2), (3, 2), (2, 0), (2, 3), (2, 1), (2, 2)):
        d_copy(p, q).wait_recv()
    for pair in PAIRS[4:]:
        project(pair)

    moe_scale = lax.rsqrt(
        jnp.sum(squares[...], axis=1, keepdims=True) * (1.0 / features) + epsilon
    )
    for f in range(tp_size):
        columns = slice(f * width, (f + 1) * width)
        normed[:, columns] = (
            hidden[:, columns].astype(F32) * moe_scale * moe_gain_ref[f : f + 1, :]
        ).astype(BF16)

    order = (2, 1, 3, 0)
    columns_of = (2, 1, 3, 0)

    def send(dy, dx):
        i = dy * SIDE + dx
        return pltpu.make_async_remote_copy(
            src_ref=outgoing.at[i], dst_ref=arrived.at[i],
            send_sem=send_sem.at[i], recv_sem=recv_sem.at[i],
            device_id=(expert_at(dy, dx), t), device_id_type=MESH,
        )

    def give_back(dy, dx):
        i = dy * SIDE + dx
        return pltpu.make_async_remote_copy(
            src_ref=results.at[i], dst_ref=returned.at[i],
            send_sem=back_send.at[i], recv_sem=back_recv.at[i],
            device_id=(expert_at(SIDE - dy, SIDE - dx), t), device_id_type=MESH,
        )

    def others(dy):
        return [dx for dx in columns_of if dy or dx]

    for dy in order:
        slot = lax.broadcasted_iota(jnp.int32, (SIDE, slots, block), 1)
        dx = lax.broadcasted_iota(jnp.int32, (SIDE, slots, block), 0)
        key = ((((y + dy) % SIDE) * SIDE) + ((x + dx) & (SIDE - 1))) * slots + slot
        chosen = (
            ((key == first_place_r[None]) | (key == second_place_r[None]))
            .astype(F32)
            .reshape(SIDE * slots, block)
            .astype(BF16)
        )
        low = jnp.dot(chosen, normed[:, :half], preferred_element_type=F32)
        high = jnp.dot(chosen, normed[:, half:], preferred_element_type=F32)
        slab = jnp.concatenate(
            [low.reshape(SIDE, slots, half), high.reshape(SIDE, slots, half)], axis=1
        ).astype(BF16)
        if dy == 0:
            arrived[0] = slab[0]
            outgoing[1:SIDE] = slab[1:]
        else:
            outgoing[dy * SIDE : (dy + 1) * SIDE] = slab
        for dx in others(dy):
            send(dy, dx).start()

    group_logits = lax.dot_general(
        normed[...], group_router_ref[...], contract_last, preferred_element_type=F32
    )
    expert_logits = lax.dot_general(
        normed[...], expert_router_ref[...], contract_last, preferred_element_type=F32
    )
    e_lane = lax.broadcasted_iota(jnp.int32, (block, experts), 1)
    groups = group_router_ref.shape[0]
    per_group = experts // groups
    group_exp = jnp.exp(group_logits)
    g_lane = lax.broadcasted_iota(jnp.int32, (block, groups), 1)
    in_group = (first >= g_lane * per_group) & (first < (g_lane + 1) * per_group)
    group_prob = jnp.sum(jnp.where(in_group, group_exp, 0.0), axis=1, keepdims=True) / jnp.sum(
        group_exp, axis=1, keepdims=True
    )
    first_exp = jnp.exp(jnp.sum(jnp.where(first == e_lane, expert_logits, 0.0), axis=1, keepdims=True))
    second_exp = jnp.exp(
        jnp.sum(jnp.where(second == e_lane, expert_logits, 0.0), axis=1, keepdims=True)
    )
    first_weight = group_prob * first_exp / (first_exp + second_exp)
    second_weight = group_prob * second_exp / (first_exp + second_exp)

    for copy in fetch_experts:
        copy.wait()
    for dy in order:
        for dx in others(dy):
            send(dy, dx).wait()
        slab = arrived[dy * SIDE : (dy + 1) * SIDE].astype(F32)
        low = slab[:, :slots].reshape(SIDE * slots, half).astype(BF16)
        high = slab[:, slots:].reshape(SIDE * slots, half).astype(BF16)
        gated = jnp.dot(low, gate_w[:half], preferred_element_type=F32) + jnp.dot(
            high, gate_w[half:], preferred_element_type=F32
        )
        upped = jnp.dot(low, up_w[:half], preferred_element_type=F32) + jnp.dot(
            high, up_w[half:], preferred_element_type=F32
        )
        inner = (jax.nn.silu(gated) * upped).astype(BF16)
        low = jnp.dot(inner, down_w[:, :half], preferred_element_type=F32)
        high = jnp.dot(inner, down_w[:, half:], preferred_element_type=F32)
        slab = jnp.concatenate(
            [low.reshape(SIDE, slots, half), high.reshape(SIDE, slots, half)], axis=1
        ).astype(BF16)
        if dy == 0:
            returned[0] = slab[0]
            results[1:SIDE] = slab[1:]
        else:
            results[dy * SIDE : (dy + 1) * SIDE] = slab
        for dx in others(dy):
            give_back(dy, dx).start()

    j = lax.broadcasted_iota(jnp.int32, (block, sp_size * slots), 1)
    i = (j * 2731) >> 16
    key = (
        ((y + (i >> 2)) & (SIDE - 1)) * SIDE + ((x + (i & (SIDE - 1))) & (SIDE - 1))
    ) * slots + (j - i * slots)
    first_hot = (key == first_place).astype(BF16)
    second_hot = (key == second_place).astype(BF16)
    for dy in order:
        for dx in others(dy):
            give_back(dy, dx).wait()

    quarter = half // 4
    for h in range(2):
        for f in range(4):
            part = returned[:, h * slots : (h + 1) * slots, f * quarter : (f + 1) * quarter]
            part = part.astype(F32).reshape(sp_size * slots, quarter).astype(BF16)
            columns = slice(h * half + f * quarter, h * half + (f + 1) * quarter)
            mixed = first_weight * jnp.dot(
                first_hot, part, preferred_element_type=F32
            ) + second_weight * jnp.dot(second_hot, part, preferred_element_type=F32)
            out_ref[:, columns] = (hidden[:, columns].astype(F32) + mixed).astype(BF16)

    for i in range(tp_size - 1):
        exchange(i).wait_send()
    for h in range(1, planes):
        z_copy(h).wait_send()
    for k in range(4):
        for n in range(pieces_of(0, k)):
            a_copy(k, n).wait_send()
    for q in range(SIDE):
        for k in range(4):
            for n in range(pieces_of(q, k)):
                b_copy(q, k, n).wait_send()
    for p in range(SIDE):
        for q in range(SIDE):
            d_copy(p, q).wait_send()


def body(
    mesh, conv_value, conv_gate, doc_ids, conv_kernel, norm_gain_conv, norm_bias_conv,
    proj_weight, residual, norm_gain_moe, group_router, expert_router, routing,
    expert_gate_w, expert_up_w, expert_down_w,
):
    sp_size, tp_size = mesh.shape["sp"], mesh.shape["tp"]
    rows, width = conv_value.shape
    block = rows // tp_size
    features = tp_size * width
    taps = conv_kernel.shape[0]
    inner = expert_gate_w.shape[2]
    slots = 2 * block // sp_size
    planes = tp_size // 2
    vmem = pl.BlockSpec(memory_space=pltpu.VMEM)
    hbm = pl.BlockSpec(memory_space=pl.ANY)
    slab = (sp_size, 2 * slots, features // 2)
    dma = pltpu.SemaphoreType.DMA
    return pl.pallas_call(
        functools.partial(layer_kernel, sp_size, tp_size),
        out_shape=jax.ShapeDtypeStruct((block, features), BF16),
        in_specs=[hbm, hbm, vmem, vmem, vmem, vmem, hbm, hbm, vmem, vmem, vmem, vmem, hbm, hbm, hbm],
        out_specs=vmem,
        scratch_shapes=[
            pltpu.VMEM((rows, width), BF16),
            pltpu.VMEM((rows, width), BF16),
            pltpu.VMEM((block, features), BF16),
            pltpu.VMEM((rows + 32, width), F32),
            pltpu.VMEM((rows, width), F32),
            pltpu.VMEM((rows // 128, 128), F32),
            pltpu.VMEM((tp_size, block, width), BF16),
            pltpu.VMEM((tp_size, block, width), BF16),
            pltpu.VMEM((8, 128), jnp.int32),
            pltpu.VMEM((taps, 8, width), F32),
            pltpu.VMEM((width, width), BF16),
            pltpu.VMEM((SIDE, SIDE, planes, width, width), BF16),
            pltpu.VMEM((SIDE, SIDE, planes, width, width), BF16),
            pltpu.VMEM((features, inner), BF16),
            pltpu.VMEM((features, inner), BF16),
            pltpu.VMEM((inner, features), BF16),
            pltpu.VMEM((2, block, features // 2), BF16),
            pltpu.VMEM((block, features), BF16),
            pltpu.VMEM((block, features), BF16),
            pltpu.VMEM((block, 128), F32),
            pltpu.VMEM(slab, BF16),
            pltpu.VMEM(slab, BF16),
            pltpu.VMEM(slab, BF16),
            pltpu.VMEM(slab, BF16),
            dma((6,)), dma((SIDE, SIDE)), dma((3,)), dma((tp_size,)), dma((tp_size,)), dma((2,)), dma((2,)),
            dma((planes,)), dma((planes,)), dma((4, 3)), dma((4, 3)),
            dma((SIDE, 4, 3)), dma((SIDE, 4, 3)), dma((SIDE, SIDE)), dma((SIDE, SIDE)),
            dma((sp_size,)), dma((sp_size,)), dma((sp_size,)), dma((sp_size,)),
        ],
        compiler_params=pltpu.CompilerParams(collective_id=0, has_side_effects=True),
    )(
        conv_value, conv_gate, doc_ids.reshape(rows // 128, 128), conv_kernel,
        norm_gain_conv.reshape(tp_size, width), norm_bias_conv.reshape(tp_size, width),
        proj_weight, residual, norm_gain_moe.reshape(tp_size, width),
        group_router.T, expert_router.T, routing.T, expert_gate_w, expert_up_w, expert_down_w,
    )


def solution(mesh):
    placed = (
        P("sp", "tp"),
        P("sp", "tp"),
        P("sp"),
        P(None, "tp"),
        P(),
        P(),
        P("tp", None),
        P(("sp", "tp"), None),
        P(),
        P(),
        P(),
        P(("sp", "tp"), None),
        P("sp", None, None),
        P("sp", None, None),
        P("sp", None, None),
    )
    return jax.shard_map(
        functools.partial(body, mesh), mesh=mesh, in_specs=placed, out_specs=P(("sp", "tp"), None), check_vma=False
    )
```

```python
import functools
import jax
import jax.numpy as jnp
from jax import lax
from jax.experimental import pallas as pl
from jax.experimental.pallas import tpu as pltpu
from jax.sharding import PartitionSpec as P

epsilon = 1e-06
MESH = pl.DeviceIdType.MESH
F32 = jnp.float32
BF16 = jnp.bfloat16
SIDE = 4
HOPS = (0, 1, 7, 2, 6, 3, 5, 4)
PIECES = ((1, 2), (3, 2), (5, 3))
PAIRS = (
    ((0, 0), (0, 1)), ((0, 3), (1, 0)), ((3, 0), (1, 1)), ((1, 3), (3, 1)),
    ((3, 3), (0, 2)), ((2, 0), (1, 2)), ((2, 1), (3, 2)), ((2, 3), (2, 2)),
)


def layer_kernel(
    sp_size, tp_size,
    value_hbm, gate_hbm, ids_ref, taps_ref, gain_ref, bias_ref, proj_hbm, residual_hbm,
    moe_gain_ref, group_router_ref, expert_router_ref, routed_ref, gate_hbm_w, up_hbm_w, down_hbm_w,
    out_ref,
    value_ref, gate_ref, residual_ref, gated, reach, compact, conv_out, raw, halo_ids, taps_wide,
    first_w, own_w, far_w, gate_w, up_w, down_w, activated, hidden, normed, mixture, squares,
    outgoing, arrived, results, returned,
    local_sem, rows_sem, expert_sem, conv_send, conv_recv, halo_send, halo_recv,
    z_send, z_recv, a_send, a_recv, b_send, b_recv, d_send, d_recv,
    send_sem, recv_sem, back_send, back_recv,
):
    s = lax.axis_index("sp")
    t = lax.axis_index("tp")
    y, x = s // SIDE, s % SIDE
    planes = tp_size // 2
    z, core = t // 2, t % 2
    rows, width = value_ref.shape
    block = rows // tp_size
    taps = taps_ref.shape[0]
    features = tp_size * width
    half = features // 2
    slots = outgoing.shape[1] // 2
    after, before = (s + 1) % sp_size, (s + sp_size - 1) % sp_size
    chunks = rows // 128

    barrier = pltpu.get_barrier_semaphore()

    def greet(i, carry):
        pl.semaphore_signal(
            barrier, inc=1, device_id=(s, (t + 1 + i) % tp_size), device_id_type=MESH
        )
        return carry

    def greet_plane(i, carry):
        pl.semaphore_signal(
            barrier, inc=1, device_id=((s + 1 + i) % sp_size, t), device_id_type=MESH
        )
        return carry

    lax.fori_loop(0, tp_size - 1, greet, 0)
    lax.fori_loop(0, sp_size - 1, greet_plane, 0)

    def expert_at(dy, dx):
        return ((y + dy) % SIDE) * SIDE + (x + dx) % SIDE

    def block_at(p, q):
        dy = (1 - core) * p + core * q
        dx = (1 - core) * q + core * p
        return expert_at(dy, dx)

    head = rows - 128
    local = [
        pltpu.make_async_copy(value_hbm.at[pl.ds(head, 128)], value_ref.at[pl.ds(head, 128)], local_sem.at[0]),
        pltpu.make_async_copy(gate_hbm.at[pl.ds(head, 128)], gate_ref.at[pl.ds(head, 128)], local_sem.at[1]),
        pltpu.make_async_copy(
            proj_hbm.at[:, pl.ds(pl.multiple_of(s * width, width), width)], first_w, local_sem.at[2]
        ),
        pltpu.make_async_copy(value_hbm.at[pl.ds(0, head)], value_ref.at[pl.ds(0, head)], local_sem.at[3]),
        pltpu.make_async_copy(gate_hbm.at[pl.ds(0, head)], gate_ref.at[pl.ds(0, head)], local_sem.at[4]),
        pltpu.make_async_copy(residual_hbm, residual_ref, local_sem.at[5]),
    ]
    for copy in local:
        copy.start()

    def own_rows(p, q):
        return pltpu.make_async_copy(
            proj_hbm.at[:, pl.ds(pl.multiple_of(block_at(p, q) * width, width), width)],
            own_w.at[p, q, 0], rows_sem.at[p, q],
        )

    for p in range(SIDE):
        for q in range(SIDE):
            own_rows(p, q).start()
    fetch_experts = [
        pltpu.make_async_copy(source.at[0], target, expert_sem.at[i])
        for i, (source, target) in enumerate(
            ((gate_hbm_w, gate_w), (up_hbm_w, up_w), (down_hbm_w, down_w))
        )
    ]
    for copy in fetch_experts:
        copy.start()

    def gate_rows(at, size):
        v = value_ref[pl.ds(at, size), :].astype(F32)
        g = gate_ref[pl.ds(at, size), :].astype(F32)
        gated[pl.ds(at + 32, size), :] = (v * jax.nn.sigmoid(g)).astype(BF16).astype(F32)

    local[0].wait()
    local[1].wait()
    gate_rows(head, 128)

    ids = ids_ref[...]
    lane = lax.broadcasted_iota(jnp.int32, (chunks, 128), 1)
    row = lax.broadcasted_iota(jnp.int32, (chunks, 128), 0)
    position = row * 128 + lane
    ones = jnp.ones((128, 128), BF16)
    below = jnp.concatenate(
        [jnp.sum((ids < d).astype(F32), axis=0, keepdims=True) for d in range(16)], axis=0
    )
    counts = jnp.dot(below.astype(BF16), ones, preferred_element_type=F32).astype(jnp.int32)
    began = jnp.zeros((chunks, 128), jnp.int32)
    for d in range(1, 16):
        began = jnp.where(ids == d, counts[d : d + 1, :], began)
    compact[...] = jnp.minimum(position - began, taps).astype(F32)
    eye = (
        lax.broadcasted_iota(jnp.int32, (128, 128), 0)
        == lax.broadcasted_iota(jnp.int32, (128, 128), 1)
    ).astype(F32)

    def widen(r, size):
        spread = [(eye * compact[pl.ds(r + n, 1), :]).astype(BF16) for n in range(size)]
        reach[pl.ds(pl.multiple_of(r * 128, 128), 128 * size), :] = jnp.dot(
            jnp.concatenate(spread, axis=0), ones, preferred_element_type=F32
        )

    def z_copy(h):
        return pltpu.make_async_remote_copy(
            src_ref=first_w, dst_ref=own_w.at[0, 0, HOPS.index(planes - h)],
            send_sem=z_send.at[h], recv_sem=z_recv.at[planes - h],
            device_id=(s, ((z + h) % planes) * 2 + core), device_id_type=MESH,
        )

    def z_arrival(h):
        return pltpu.make_async_remote_copy(
            src_ref=first_w, dst_ref=own_w.at[0, 0, HOPS.index(h)],
            send_sem=z_send.at[h], recv_sem=z_recv.at[h],
            device_id=(s, ((z + h) % planes) * 2 + core), device_id_type=MESH,
        )

    local[2].wait()
    pl.semaphore_wait(barrier, tp_size + sp_size - 2)
    for h in HOPS[1:]:
        z_copy(h).start()
    halo_id = pltpu.make_async_remote_copy(
        src_ref=ids_ref.at[pl.ds(chunks - 8, 8)], dst_ref=halo_ids,
        send_sem=halo_send.at[1], recv_sem=halo_recv.at[1],
        device_id=(after, t), device_id_type=MESH,
    )
    halo_id.start()
    halo = pltpu.make_async_remote_copy(
        src_ref=gated.at[pl.ds(rows, 32)], dst_ref=gated.at[pl.ds(0, 32)],
        send_sem=halo_send.at[0], recv_sem=halo_recv.at[0],
        device_id=(after, t), device_id_type=MESH,
    )
    halo.start()

    def widen_step(r, carry):
        widen(r * 8, 8)
        return carry

    lax.fori_loop(0, chunks // 8, widen_step, 0)
    wide = taps_ref[...].astype(F32)
    for k in range(taps):
        taps_wide[k] = jnp.broadcast_to(wide[k : k + 1, :], (8, width))
    local[3].wait()
    local[4].wait()
    gate_rows(head - 256, 256)

    def gate_step(r, carry):
        gate_rows(pl.multiple_of(r * 384, 128), 384)
        return carry

    lax.fori_loop(0, (head - 256) // 384, gate_step, 0)

    def receive_halo():
        halo_id.wait()
        tail_lane = lax.broadcasted_iota(jnp.int32, (1, 128), 1)
        shared = (halo_ids[7:8, :] == ids_ref[0:1, 0:1]) & (tail_lane >= 128 - (taps - 1))
        extra = jnp.sum(shared.astype(F32), axis=1, keepdims=True)
        extra = extra * (s > 0).astype(F32)
        place = lax.broadcasted_iota(jnp.int32, (1, 128), 1).astype(F32)
        near = compact[0:1, :]
        joined = (near == place).astype(F32)
        compact[0:1, :] = jnp.minimum(near + joined * extra, float(taps))
        widen(0, 1)
        halo.wait()

    def along_q(d):
        return (1 - core) * (y * SIDE + (x + d) % SIDE) + core * (((y + d) % SIDE) * SIDE + x)

    def along_p(d):
        return core * (y * SIDE + (x + d) % SIDE) + (1 - core) * (((y + d) % SIDE) * SIDE + x)

    rest, lower, upper = pl.ds(1, 7), pl.ds(1, 4), pl.ds(5, 3)

    def remote(source, target, send, recv, to):
        return pltpu.make_async_remote_copy(
            src_ref=source, dst_ref=target, send_sem=send, recv_sem=recv,
            device_id=(to, t), device_id_type=MESH,
        )

    def a_copy(k, n=0):
        cut = pl.ds(*PIECES[n]) if k < 2 else (lower, upper)[k - 2]
        origin, landing, to = ((0, 3, 1), (0, 1, 3), (3, 2, 1), (1, 2, 3))[k]
        return remote(
            own_w.at[0, origin, cut], own_w.at[0, landing, cut],
            a_send.at[k, n], a_recv.at[k, n], along_q(to),
        )

    def b_copy(q, k, n=0):
        cut = (pl.ds(*PIECES[n]) if q == 0 else rest) if k < 2 else (lower, upper)[k - 2]
        origin, landing, to = ((0, 3, 1), (0, 1, 3), (3, 2, 1), (1, 2, 3))[k]
        return remote(
            own_w.at[origin, q, cut], own_w.at[landing, q, cut],
            b_send.at[q, k, n], b_recv.at[q, k, n], along_p(to),
        )

    def pieces_of(q, k):
        return len(PIECES) if k < 2 and q == 0 else 1

    def d_copy(p, q):
        return pltpu.make_async_remote_copy(
            src_ref=own_w.at[p, q], dst_ref=far_w.at[p, q],
            send_sem=d_send.at[p, q], recv_sem=d_recv.at[p, q],
            device_id=(s, z * 2 + 1 - core), device_id_type=MESH,
        )

    def open_gather(n):
        for m in range(PIECES[n][0], PIECES[n][0] + PIECES[n][1]):
            z_arrival(HOPS[m]).wait_recv()
        a_copy(0, n).start()
        a_copy(1, n).start()
        b_copy(0, 0, n).start()
        b_copy(0, 1, n).start()
        if n == len(PIECES) - 1:
            own_rows(0, 0).wait()
            d_copy(0, 0).start()

    tile = 32

    def conv_block(b, store):
        def conv_tile(q, carry):
            base = pl.multiple_of(b * block + q * tile, tile)
            limit = reach[pl.ds(base, tile), :].reshape(tile // 8, 8, width)
            total = jnp.zeros((tile // 8, 8, width), F32)
            for k in range(taps):
                j = taps - 1 - k
                v = gated[pl.ds(base + (32 - j), tile), :].reshape(tile // 8, 8, width)
                total = total + jnp.where(limit >= j, v * taps_wide[k][None], 0.0)
            store(pl.multiple_of(q * tile, tile), total.reshape(tile, width).astype(BF16))
            return carry

        lax.fori_loop(0, block // tile, conv_tile, 0)

    def rank(i):
        k = i // 2
        size = planes // 2 - (k + 1) // 2
        hop = (k % 2) * size + (1 - k % 2) * (planes - size)
        return ((z + hop) % planes) * 2 + (core + 1 + i) % 2

    early = rank(14)
    met = sum((rank(i) == 0).astype(jnp.int32) for i in range(14))

    def flag(truth):
        return int(truth) if isinstance(truth, bool) else truth.astype(jnp.int32)

    def target(i):
        to = rank(i)
        first = (to == 0).astype(jnp.int32) * flag(i < 14)
        swap = flag(i == 14)
        return (to + first * early) * (1 - swap * met)

    def exchange(i):
        to = target(i)
        return pltpu.make_async_remote_copy(
            src_ref=conv_out.at[to], dst_ref=raw.at[t],
            send_sem=conv_send.at[i], recv_sem=conv_recv.at[t],
            device_id=(s, to), device_id_type=MESH,
        )

    def step(i, carry):
        b = target(i)

        @pl.when(i == 14)
        def _():
            receive_halo()

        def store(at, value):
            conv_out[b, pl.ds(at, tile), :] = value

        conv_block(b, store)

        @pl.when(i > 0)
        def _():
            exchange(i - 1).start()

        for n, at in enumerate((4, 8, 12)):

            @pl.when(i == at)
            def _(n=n):
                open_gather(n)

        return carry

    lax.fori_loop(0, tp_size - 1, step, 0)

    def store_own(at, value):
        raw[t, pl.ds(at, tile), :] = value

    conv_block(t, store_own)
    exchange(tp_size - 2).start()

    for k in range(2):
        for n in range(len(PIECES)):
            a_copy(k, n).wait_recv()
    for k in (2, 3):
        a_copy(k).start()
    for q in (3, 1):
        b_copy(q, 0).start()
        b_copy(q, 1).start()
        own_rows(0, q).wait()
        d_copy(0, q).start()

    experts = expert_router_ref.shape[0]
    e_row = lax.broadcasted_iota(jnp.int32, (experts, block), 0)
    first_r, second_r = routed_ref[0:1, :], routed_ref[1:2, :]
    pick_first_r, pick_second_r = first_r == e_row, second_r == e_row
    named_r = (pick_first_r | pick_second_r).astype(F32)
    token_r = lax.broadcasted_iota(jnp.int32, (block, block), 0)
    token_c = lax.broadcasted_iota(jnp.int32, (block, block), 1)
    earlier_r = jnp.dot(
        named_r.astype(BF16), (token_r < token_c).astype(BF16), preferred_element_type=F32
    )
    first_rank = jnp.sum(jnp.where(pick_first_r, earlier_r, 0.0), axis=0, keepdims=True)
    second_rank = jnp.sum(jnp.where(pick_second_r, earlier_r, 0.0), axis=0, keepdims=True)
    first_place_r = first_r * slots + first_rank.astype(jnp.int32)
    second_place_r = second_r * slots + second_rank.astype(jnp.int32)
    standing = jnp.concatenate(
        [
            first_r.astype(F32), second_r.astype(F32), first_rank, second_rank,
            jnp.zeros((4, block), F32),
        ],
        axis=0,
    ).astype(BF16)
    contract_last = (((1,), (1,)), ((), ()))
    turned = lax.dot_general(
        (token_r == token_c).astype(BF16), standing, contract_last, preferred_element_type=F32
    ).astype(jnp.int32)
    first, second = turned[:, 0:1], turned[:, 1:2]
    first_place = first * slots + turned[:, 2:3]
    second_place = second * slots + turned[:, 3:4]

    for k in (2, 3):
        a_copy(k).wait_recv()
    b_copy(2, 0).start()
    b_copy(2, 1).start()
    own_rows(0, 2).wait()
    d_copy(0, 2).start()

    def relay(q):
        for k in range(2):
            for n in range(pieces_of(q, k)):
                b_copy(q, k, n).wait_recv()
        b_copy(q, 2).start()
        b_copy(q, 3).start()
        for p in (3, 1):
            own_rows(p, q).wait()
            d_copy(p, q).start()

    def close(q):
        b_copy(q, 2).wait_recv()
        b_copy(q, 3).wait_recv()
        own_rows(2, q).wait()
        d_copy(2, q).start()

    for q in (0, 3, 1):
        relay(q)

    def conv_arrival(i, carry):
        source = (t + 1 + i) % tp_size
        pltpu.make_async_remote_copy(
            src_ref=conv_out.at[source], dst_ref=raw.at[source],
            send_sem=conv_send.at[i], recv_sem=conv_recv.at[source],
            device_id=(s, source), device_id_type=MESH,
        ).wait_recv()
        return carry

    lax.fori_loop(0, tp_size - 1, conv_arrival, 0)

    def activate(r, carry):
        at = pl.multiple_of(r * 48, 48)
        v = raw[:, pl.ds(at, 48), :].astype(F32)
        average = jnp.sum(jnp.sum(v, axis=0), axis=1, keepdims=True) * (1.0 / features)
        centered = v - average[None]
        variance = jnp.sum(jnp.sum(centered * centered, axis=0), axis=1, keepdims=True) * (
            1.0 / features
        )
        scale = lax.rsqrt(variance + epsilon)
        for m in range(planes):
            for side in range(2):
                b = ((z + HOPS[m]) % planes) * 2 + side
                u = raw[b, pl.ds(at, 48), :].astype(F32) - average
                u = u * scale * gain_ref[pl.ds(b, 1), :] + bias_ref[pl.ds(b, 1), :]
                activated[side, pl.ds(at, 48), m * width : (m + 1) * width] = (
                    jax.nn.silu(u).astype(BF16)
                )
        return carry

    lax.fori_loop(0, block // 48, activate, 0)
    for q in (2,):
        relay(q)

    squares[...] = jnp.zeros_like(squares)
    local[5].wait()

    def project(pair):
        def column(source, swap):
            parts = []
            for dy, dx in pair:
                i = dy * (1 - swap) + dx * swap
                k = dx * (1 - swap) + dy * swap
                parts.append(source[i, k].reshape(planes * width, width))
            return jnp.concatenate(parts, axis=1)

        total = jnp.dot(
            activated[core], column(own_w, core), preferred_element_type=F32
        ) + jnp.dot(activated[1 - core], column(far_w, 1 - core), preferred_element_type=F32)
        for n, (dy, dx) in enumerate(pair):
            columns = pl.ds(pl.multiple_of(expert_at(dy, dx) * width, width), width)
            state = (
                residual_ref[:, columns].astype(F32) + total[:, n * width : (n + 1) * width]
            ).astype(BF16)
            hidden[:, columns] = state
            wide_state = state.astype(F32)
            squares[...] += wide_state * wide_state

    near = (0, 1, 3)
    for p in near:
        for q in near:
            d_copy(p, q).wait_recv()
    for pair in PAIRS[:2]:
        project(pair)
    for q in (0, 3):
        close(q)
    for pair in PAIRS[2:4]:
        project(pair)
    for q in (1, 2):
        close(q)
    for p, q in ((0, 2), (1, 2), (3, 2), (2, 0), (2, 3), (2, 1), (2, 2)):
        d_copy(p, q).wait_recv()
    for pair in PAIRS[4:]:
        project(pair)

    moe_scale = lax.rsqrt(
        jnp.sum(squares[...], axis=1, keepdims=True) * (1.0 / features) + epsilon
    )
    for f in range(tp_size):
        columns = slice(f * width, (f + 1) * width)
        normed[:, columns] = (
            hidden[:, columns].astype(F32) * moe_scale * moe_gain_ref[f : f + 1, :]
        ).astype(BF16)

    order = (1, 3, 2, 0)
    columns_of = (2, 1, 3, 0)

    def send(dy, dx):
        i = dy * SIDE + dx
        return pltpu.make_async_remote_copy(
            src_ref=outgoing.at[i], dst_ref=arrived.at[i],
            send_sem=send_sem.at[i], recv_sem=recv_sem.at[i],
            device_id=(expert_at(dy, dx), t), device_id_type=MESH,
        )

    def give_back(dy, dx):
        i = dy * SIDE + dx
        return pltpu.make_async_remote_copy(
            src_ref=results.at[i], dst_ref=returned.at[i],
            send_sem=back_send.at[i], recv_sem=back_recv.at[i],
            device_id=(expert_at(SIDE - dy, SIDE - dx), t), device_id_type=MESH,
        )

    def others(dy):
        return [dx for dx in columns_of if dy or dx]

    for dy in order:
        slot = lax.broadcasted_iota(jnp.int32, (SIDE, slots, block), 1)
        dx = lax.broadcasted_iota(jnp.int32, (SIDE, slots, block), 0)
        key = ((((y + dy) % SIDE) * SIDE) + ((x + dx) & (SIDE - 1))) * slots + slot
        chosen = (
            ((key == first_place_r[None]) | (key == second_place_r[None]))
            .astype(F32)
            .reshape(SIDE * slots, block)
            .astype(BF16)
        )
        low = jnp.dot(chosen, normed[:, :half], preferred_element_type=F32)
        high = jnp.dot(chosen, normed[:, half:], preferred_element_type=F32)
        slab = jnp.concatenate(
            [low.reshape(SIDE, slots, half), high.reshape(SIDE, slots, half)], axis=1
        ).astype(BF16)
        if dy == 0:
            arrived[0] = slab[0]
            outgoing[1:SIDE] = slab[1:]
        else:
            outgoing[dy * SIDE : (dy + 1) * SIDE] = slab
        for dx in others(dy):
            send(dy, dx).start()

    group_logits = lax.dot_general(
        normed[...], group_router_ref[...], contract_last, preferred_element_type=F32
    )
    expert_logits = lax.dot_general(
        normed[...], expert_router_ref[...], contract_last, preferred_element_type=F32
    )
    e_lane = lax.broadcasted_iota(jnp.int32, (block, experts), 1)
    groups = group_router_ref.shape[0]
    per_group = experts // groups
    group_exp = jnp.exp(group_logits)
    g_lane = lax.broadcasted_iota(jnp.int32, (block, groups), 1)
    in_group = (first >= g_lane * per_group) & (first < (g_lane + 1) * per_group)
    group_prob = jnp.sum(jnp.where(in_group, group_exp, 0.0), axis=1, keepdims=True) / jnp.sum(
        group_exp, axis=1, keepdims=True
    )
    first_exp = jnp.exp(jnp.sum(jnp.where(first == e_lane, expert_logits, 0.0), axis=1, keepdims=True))
    second_exp = jnp.exp(
        jnp.sum(jnp.where(second == e_lane, expert_logits, 0.0), axis=1, keepdims=True)
    )
    first_weight = group_prob * first_exp / (first_exp + second_exp)
    second_weight = group_prob * second_exp / (first_exp + second_exp)

    for copy in fetch_experts:
        copy.wait()
    for dy in order:
        for dx in others(dy):
            send(dy, dx).wait()
        slab = arrived[dy * SIDE : (dy + 1) * SIDE].astype(F32)
        low = slab[:, :slots].reshape(SIDE * slots, half).astype(BF16)
        high = slab[:, slots:].reshape(SIDE * slots, half).astype(BF16)
        gated = jnp.dot(low, gate_w[:half], preferred_element_type=F32) + jnp.dot(
            high, gate_w[half:], preferred_element_type=F32
        )
        upped = jnp.dot(low, up_w[:half], preferred_element_type=F32) + jnp.dot(
            high, up_w[half:], preferred_element_type=F32
        )
        inner = (jax.nn.silu(gated) * upped).astype(BF16)
        low = jnp.dot(inner, down_w[:, :half], preferred_element_type=F32)
        high = jnp.dot(inner, down_w[:, half:], preferred_element_type=F32)
        slab = jnp.concatenate(
            [low.reshape(SIDE, slots, half), high.reshape(SIDE, slots, half)], axis=1
        ).astype(BF16)
        if dy == 0:
            returned[0] = slab[0]
            results[1:SIDE] = slab[1:]
        else:
            results[dy * SIDE : (dy + 1) * SIDE] = slab
        for dx in others(dy):
            give_back(dy, dx).start()

    def hot(dy):
        j = lax.broadcasted_iota(jnp.int32, (block, SIDE * slots), 1)
        i = (j * 2731) >> 16
        key = (((y + dy) % SIDE) * SIDE + ((x + i) & (SIDE - 1))) * slots + (j - i * slots)
        return (key == first_place).astype(BF16), (key == second_place).astype(BF16)

    hots = [hot(dy) for dy in order]
    quarter = half // 4
    for n, dy in enumerate(order):
        for dx in others(dy):
            give_back(dy, dx).wait()
        first_part, second_part = hots[n]
        for h in range(2):
            for f in range(4):
                part = returned[
                    dy * SIDE : (dy + 1) * SIDE,
                    h * slots : (h + 1) * slots, f * quarter : (f + 1) * quarter,
                ]
                part = part.astype(F32).reshape(SIDE * slots, quarter).astype(BF16)
                columns = slice(h * half + f * quarter, h * half + (f + 1) * quarter)
                mixed = first_weight * jnp.dot(
                    first_part, part, preferred_element_type=F32
                ) + second_weight * jnp.dot(second_part, part, preferred_element_type=F32)
                if n == 0:
                    mixture[:, columns] = mixed
                elif n < len(order) - 1:
                    mixture[:, columns] += mixed
                else:
                    out_ref[:, columns] = (
                        hidden[:, columns].astype(F32) + (mixture[:, columns] + mixed)
                    ).astype(BF16)

    for i in range(tp_size - 1):
        exchange(i).wait_send()
    for h in range(1, planes):
        z_copy(h).wait_send()
    for k in range(4):
        for n in range(pieces_of(0, k)):
            a_copy(k, n).wait_send()
    for q in range(SIDE):
        for k in range(4):
            for n in range(pieces_of(q, k)):
                b_copy(q, k, n).wait_send()
    for p in range(SIDE):
        for q in range(SIDE):
            d_copy(p, q).wait_send()


def body(
    mesh, conv_value, conv_gate, doc_ids, conv_kernel, norm_gain_conv, norm_bias_conv,
    proj_weight, residual, norm_gain_moe, group_router, expert_router, routing,
    expert_gate_w, expert_up_w, expert_down_w,
):
    sp_size, tp_size = mesh.shape["sp"], mesh.shape["tp"]
    rows, width = conv_value.shape
    block = rows // tp_size
    features = tp_size * width
    taps = conv_kernel.shape[0]
    inner = expert_gate_w.shape[2]
    slots = 2 * block // sp_size
    planes = tp_size // 2
    vmem = pl.BlockSpec(memory_space=pltpu.VMEM)
    hbm = pl.BlockSpec(memory_space=pl.ANY)
    slab = (sp_size, 2 * slots, features // 2)
    dma = pltpu.SemaphoreType.DMA
    return pl.pallas_call(
        functools.partial(layer_kernel, sp_size, tp_size),
        out_shape=jax.ShapeDtypeStruct((block, features), BF16),
        in_specs=[hbm, hbm, vmem, vmem, vmem, vmem, hbm, hbm, vmem, vmem, vmem, vmem, hbm, hbm, hbm],
        out_specs=vmem,
        scratch_shapes=[
            pltpu.VMEM((rows, width), BF16),
            pltpu.VMEM((rows, width), BF16),
            pltpu.VMEM((block, features), BF16),
            pltpu.VMEM((rows + 32, width), F32),
            pltpu.VMEM((rows, width), F32),
            pltpu.VMEM((rows // 128, 128), F32),
            pltpu.VMEM((tp_size, block, width), BF16),
            pltpu.VMEM((tp_size, block, width), BF16),
            pltpu.VMEM((8, 128), jnp.int32),
            pltpu.VMEM((taps, 8, width), F32),
            pltpu.VMEM((width, width), BF16),
            pltpu.VMEM((SIDE, SIDE, planes, width, width), BF16),
            pltpu.VMEM((SIDE, SIDE, planes, width, width), BF16),
            pltpu.VMEM((features, inner), BF16),
            pltpu.VMEM((features, inner), BF16),
            pltpu.VMEM((inner, features), BF16),
            pltpu.VMEM((2, block, features // 2), BF16),
            pltpu.VMEM((block, features), BF16),
            pltpu.VMEM((block, features), BF16),
            pltpu.VMEM((block, features), F32),
            pltpu.VMEM((block, 128), F32),
            pltpu.VMEM(slab, BF16),
            pltpu.VMEM(slab, BF16),
            pltpu.VMEM(slab, BF16),
            pltpu.VMEM(slab, BF16),
            dma((6,)), dma((SIDE, SIDE)), dma((3,)), dma((tp_size,)), dma((tp_size,)), dma((2,)), dma((2,)),
            dma((planes,)), dma((planes,)), dma((4, 3)), dma((4, 3)),
            dma((SIDE, 4, 3)), dma((SIDE, 4, 3)), dma((SIDE, SIDE)), dma((SIDE, SIDE)),
            dma((sp_size,)), dma((sp_size,)), dma((sp_size,)), dma((sp_size,)),
        ],
        compiler_params=pltpu.CompilerParams(collective_id=0, has_side_effects=True),
    )(
        conv_value, conv_gate, doc_ids.reshape(rows // 128, 128), conv_kernel,
        norm_gain_conv.reshape(tp_size, width), norm_bias_conv.reshape(tp_size, width),
        proj_weight, residual, norm_gain_moe.reshape(tp_size, width),
        group_router.T, expert_router.T, routing.T, expert_gate_w, expert_up_w, expert_down_w,
    )


def solution(mesh):
    placed = (
        P("sp", "tp"),
        P("sp", "tp"),
        P("sp"),
        P(None, "tp"),
        P(),
        P(),
        P("tp", None),
        P(("sp", "tp"), None),
        P(),
        P(),
        P(),
        P(("sp", "tp"), None),
        P("sp", None, None),
        P("sp", None, None),
        P("sp", None, None),
    )
    return jax.shard_map(
        functools.partial(body, mesh), mesh=mesh, in_specs=placed, out_specs=P(("sp", "tp"), None), check_vma=False
    )
```
